128 devices in a mesh: grp: 4 (over y, x), ep: 32 (over z, core).
Axes of the slice: x: 2, y: 2, z: 16, core: 2. Of those that a mesh axis runs over, the one named last changes fastest.
The devices are a block of a 8x8x16 slice.
Arguments:
- tokens: bfloat16 [4096, 2048], P(('grp', 'ep')), parts along dimension 0, may hold values from -6 to 6
- norm_gain: float32 [2048], replicated, may hold values from 0.5 to 4
- routes: int32 [4096, 4], P(('grp', 'ep')), parts along dimension 0, may hold values from 0 to 31, all different within a row; in each aligned block of 32 rows (0 to 31, 32 to 63, ...) at most 8 rows name the same one
- route_logits: float32 [4096, 4], P(('grp', 'ep')), parts along dimension 0, may hold values from -6 to 6
- w_gate: bfloat16 [32, 2048, 1792], P('ep'), may hold values from -0.125 to 0.125
- w_up: bfloat16 [32, 2048, 1792], P('ep'), may hold values from -0.125 to 0.125
- w_down: bfloat16 [32, 1792, 2048], P('ep'), may hold values from -0.125 to 0.125
Outputs:
- mixed: bfloat16 [4096, 2048], P(('grp', 'ep')), parts along dimension 0
The draws below stay inside these ranges and needn't reach their ends.
There are 4 independent parts, one for each index of `grp`. The reference program is written for one: setup_inputs(seed, part) draws one part's arguments, and reference() takes and returns one part's arrays. A program takes and returns all parts, laid end to end along the dimension named above; an argument that names none is the same for every part. Nothing has to cross between parts.
Inputs may be any that keep to these rules, and one draw needn't show every extreme that they name: `routes`: each token names 4 different experts. Among the 32 tokens of one device no expert is named by more than 8 of them, and in every draw some expert is named by exactly 8 tokens of some device.
All inputs are finite; a program needn't handle non-finite values.
Results may differ from the reference program's by a relative error of at most 0.012.
Values may be sent and summed in bfloat16 or wider, within the bound.
No kernel may reach another device: no remote copies, remote signals or barrier semaphores. Data moves between devices by JAX's collectives and lax.ppermute only.
A program may use at most 64 MiB of HBM per device.

```python
import math
import jax
import jax.numpy as jnp
import numpy as np
from jax import lax

D = 2048
FF = 1792
TOP_K = 4
TOK_DEV = 32
EXPERTS = 32
CAP = 8
TOKENS = 1024


def level_of(rng, extent, cuts, low, largest):
    level, own = 1.0, jax.random.fold_in(rng, 6)
    for dim, blocks in cuts:
        draws = jnp.exp(jax.random.uniform(jax.random.fold_in(own, dim), (blocks,), jnp.float32, low / len(cuts), largest / len(cuts)))
        level = level * jnp.repeat(draws, extent[dim] // blocks).reshape([-1 if axis == dim else 1 for axis in range(len(extent))])
    return level


def deal_out(own_key, own, number, rows, amount, top, reach, slope):
    sequence = jax.random.permutation(own_key, amount)
    packed, ordinary = load_shares(amount, rows * top, reach, slope, True), load_shares(amount, rows * top, reach, slope, False)
    places = jnp.arange(amount)

    def named(tallies, turn):
        used = int((tallies > 0).sum())
        fixed = max(1, used // 4)
        moved = fixed + (places - fixed + turn * (used - fixed)) % max(1, amount - fixed)
        return jnp.zeros((amount,), jnp.int32).at[sequence[jnp.where(places < fixed, places, moved)]].set(jnp.asarray(tallies, jnp.int32))

    tallies = jnp.where(number % 4 == 0, named(packed, number // 4), named(ordinary, number - number // 4 - 1))
    mixed = jax.random.permutation(jax.random.fold_in(own, 3), amount)
    giver, receiver = mixed[0:amount // 2 * 2:2], mixed[1:amount // 2 * 2:2]
    margin = jnp.minimum(tallies[giver] - 1, reach - tallies[receiver]) // 2
    margin = jnp.where((giver == sequence[0]) | (receiver == sequence[0]) | (tallies[receiver] == 0), 0, jnp.maximum(margin, 0))
    moved = jax.random.randint(jax.random.fold_in(own, 4), (amount // 2,), 0, 1 << 20) % (margin + 1)
    tallies = tallies.at[giver].add(-moved).at[receiver].add(moved)
    items = jnp.searchsorted(jnp.cumsum(tallies), jnp.arange(rows * top), side="right").astype(jnp.int32)
    grid = items.reshape(top, rows).T
    grid = grid[jax.random.permutation(jax.random.fold_in(own, 1), rows)]
    turn = jax.random.randint(jax.random.fold_in(own, 2), (rows, 1), 0, top)
    return jnp.take_along_axis(grid, (jnp.arange(top)[None, :] + turn) % top, axis=1)


def load_shares(count, total, bound, slope, full):
    portions = [(1 << 20) // math.isqrt(rank ** slope) + 1 for rank in range(1, count + 1)]
    largest = bound if full else min(bound, max(-(-total // count), total * portions[0] // sum(portions)))
    least = 1 if total - largest >= count - 1 else 0
    given, surplus = [largest] + [least] * (count - 1), total - largest - least * (count - 1)
    while surplus > 0:
        movable = [i for i in range(1, count) if given[i] < largest] or [i for i in range(1, count) if given[i] < bound]
        pool, left = sum([portions[i] for i in movable]), surplus
        for i in movable:
            addition = min(bound - given[i], max(1, left * portions[i] // pool), surplus)
            given[i] = given[i] + addition
            surplus = surplus - addition
    return np.array(given)


def centred(stream_key, shape, scale, limit, split=(), kind=jnp.bfloat16):
    factor_of = level_of(stream_key, shape, split, -0.22, 0.18) if split else 1.0
    drawn = jax.random.normal(stream_key, shape, jnp.float32) * scale * factor_of
    return jnp.minimum(jnp.maximum(drawn, -limit), limit).astype(kind)


def setup_inputs(seed: int = 0, part: int = 0) -> dict:
    arg_keys = jax.random.split(jax.random.key(seed), 8)
    part_keys = jax.random.split(jax.random.fold_in(arg_keys[7], part), 8)
    tokens = centred(part_keys[0], (TOKENS, D), 1.0, 6.0, ((0, 32),))
    norm_gain = jnp.clip(jnp.exp(jax.random.uniform(arg_keys[1], (D,), jnp.float32, math.log(0.5), math.log(4.0))), 0.5, 4.0)
    routes_keys = jax.random.split(jax.random.fold_in(part_keys[2], 1), TOKENS // TOK_DEV)
    routes_turns = jax.random.permutation(jax.random.fold_in(part_keys[2], 3), TOKENS // TOK_DEV)
    routes = jax.vmap(lambda own, number: deal_out(jax.random.fold_in(part_keys[2], 2), own, number, TOK_DEV, EXPERTS, TOP_K, CAP, 2))(routes_keys, routes_turns).reshape((TOKENS, TOP_K))
    route_logits = centred(part_keys[3], (TOKENS, TOP_K), 1.5, 6.0, ((0, 32),), jnp.float32)
    w_gate = centred(arg_keys[4], (EXPERTS, D, FF), D ** -0.5, 0.125, ((0, 32),))
    w_up = centred(arg_keys[5], (EXPERTS, D, FF), D ** -0.5, 0.125, ((0, 32),))
    w_down = centred(arg_keys[6], (EXPERTS, FF, D), FF ** -0.5, 0.125, ((0, 32),))
    return dict(tokens=tokens, norm_gain=norm_gain, routes=routes, route_logits=route_logits, w_gate=w_gate, w_up=w_up, w_down=w_down)


def rmsnorm(values, gain):
    floats = values.astype(jnp.float32)
    scaled = floats * lax.rsqrt(lax.optimization_barrier(jnp.mean(floats * floats, axis=-1, keepdims=True)) + 1e-06)
    return (scaled * gain.astype(jnp.float32)).astype(jnp.bfloat16)

def expert(rows, gate_weight, up_weight, down_weight):
    gate = jnp.minimum(jnp.dot(rows, gate_weight, preferred_element_type=jnp.float32), 7.0)
    upper = jnp.clip(jnp.dot(rows, up_weight, preferred_element_type=jnp.float32), -7.0, 7.0)
    active = (gate * jax.nn.sigmoid(1.702 * gate) * (upper + 1.0)).astype(jnp.bfloat16)
    return jnp.dot(active, down_weight, preferred_element_type=jnp.float32).astype(jnp.bfloat16)

def reference(tokens, norm_gain, routes, route_logits, w_gate, w_up, w_down):
    normed = rmsnorm(tokens, norm_gain)
    route_weights = jax.nn.softmax(route_logits.astype(jnp.float32), axis=-1)

    def add_expert(total, expert_id):
        weight = lax.optimization_barrier(jnp.sum(jnp.where(routes == expert_id, route_weights, 0.0), axis=1))
        output = expert(normed, w_gate[expert_id], w_up[expert_id], w_down[expert_id])
        return (total + weight[:, None] * output.astype(jnp.float32), None)
    start = jnp.zeros((tokens.shape[0], tokens.shape[1]), jnp.float32)
    total, _ = lax.scan(add_expert, start, jnp.arange(EXPERTS, dtype=jnp.int32))
    return total.astype(jnp.bfloat16)
```

```python
import jax
import jax.numpy as jnp
from jax import lax
from jax.sharding import Mesh
from jax.sharding import PartitionSpec as P

TOP_K = 4
EP = ("ep_0", "ep_1")
GRP_EP = ("grp", "ep_0", "ep_1")


def rmsnorm(values, gain):
    floats = values.astype(jnp.float32)
    scaled = floats * lax.rsqrt(jnp.mean(floats * floats, axis=-1, keepdims=True) + 1e-06)
    return (scaled * gain).astype(jnp.bfloat16)


def expert(rows, gate_weight, up_weight, down_weight):
    gate = jnp.minimum(jnp.dot(rows, gate_weight, preferred_element_type=jnp.float32), 7.0)
    upper = jnp.clip(jnp.dot(rows, up_weight, preferred_element_type=jnp.float32), -7.0, 7.0)
    active = (gate * jax.nn.sigmoid(1.702 * gate) * (upper + 1.0)).astype(jnp.bfloat16)
    return jnp.dot(active, down_weight, preferred_element_type=jnp.float32).astype(jnp.bfloat16)


def shards(tokens, norm_gain, routes, route_logits, w_gate, w_up, w_down):
    tok_rows = tokens.shape[0]
    width = tokens.shape[1]
    n_experts = lax.axis_size(EP)
    capacity = max(2, 2 * tok_rows * TOP_K // n_experts)
    slot_count = n_experts * capacity
    normed = rmsnorm(tokens, norm_gain)
    route_weights = jax.nn.softmax(route_logits, axis=-1)
    slot_ids = jnp.arange(slot_count, dtype=jnp.int32)
    chosen = routes.reshape(-1)
    onehot = (chosen[:, None] == jnp.arange(n_experts, dtype=jnp.int32)[None, :]).astype(jnp.int32)
    within = jnp.sum(jnp.cumsum(onehot, axis=0) * onehot, axis=1) - 1
    slot_of = chosen * capacity + within
    placing = (slot_of[:, None] == slot_ids[None, :]).astype(jnp.bfloat16)
    repeated = jnp.repeat(normed, TOP_K, axis=0)
    outgoing = jnp.einsum("ps,pd->sd", placing, repeated, preferred_element_type=jnp.float32)
    outgoing = outgoing.astype(jnp.bfloat16).reshape(n_experts, capacity, width)
    arrived = lax.all_to_all(outgoing, EP, split_axis=0, concat_axis=0, tiled=True)
    count = arrived.shape[1]
    rows_in = arrived.reshape(n_experts * count, width)
    result = expert(rows_in, w_gate[0], w_up[0], w_down[0]).reshape(n_experts, count, width)
    returned_rows = lax.all_to_all(result, EP, split_axis=0, concat_axis=0, tiled=True)
    returned_rows = returned_rows.reshape(slot_count, width)
    picked = jnp.dot(placing, returned_rows, preferred_element_type=jnp.float32)
    total = jnp.sum(picked.reshape(tok_rows, TOP_K, width) * route_weights[:, :, None], axis=1)
    return total.astype(jnp.bfloat16)


def solution(mesh):
    split = Mesh(mesh.devices.reshape(mesh.shape["grp"], 16, 2), ("grp", "ep_0", "ep_1"))
    placed = (
        P(GRP_EP, None),
        P(),
        P(GRP_EP, None),
        P(GRP_EP, None),
        P(EP, None, None),
        P(EP, None, None),
        P(EP, None, None),
    )
    return jax.shard_map(
        shards, mesh=split, in_specs=placed, out_specs=P(GRP_EP, None), check_vma=False
    )
```

```python
import functools

import jax
import jax.numpy as jnp
from jax import lax
from jax.experimental import pallas as pl
from jax.experimental.pallas import tpu as pltpu
from jax.sharding import Mesh
from jax.sharding import PartitionSpec as P

HOP = 5
NEAR = (-2, -1, 0, 1, 2)
GRP_EP = ("grp", "z", "c")
META = 128
LIMIT = 16 << 20
VMEM = pl.BlockSpec(memory_space=pltpu.VMEM)
SMEM = pl.BlockSpec(memory_space=pltpu.SMEM)


def call(body, out_shape, n_in, smem=0, limit=LIMIT, scratch=(), flops=1 << 20):
    return pl.pallas_call(
        body,
        out_shape=out_shape,
        in_specs=[SMEM] * smem + [VMEM] * (n_in - smem),
        scratch_shapes=scratch,
        compiler_params=pltpu.CompilerParams(vmem_limit_bytes=limit),
        cost_estimate=pl.CostEstimate(flops=flops, bytes_accessed=1 << 20, transcendentals=0),
    )


def prepare(cap, tok_ref, gain_ref, routes_ref, logits_ref, out_ref):
    rows, width = tok_ref.shape
    top = routes_ref.shape[1]
    x = tok_ref[...].astype(jnp.float32)
    scale = lax.rsqrt(jnp.mean(x * x, axis=-1, keepdims=True) + 1e-06)
    out_ref[:, :width] = (x * scale * gain_ref[...]).astype(jnp.bfloat16)
    lane = lax.broadcasted_iota(jnp.int32, (rows, META), 1)
    routes = routes_ref[...]
    named = jnp.zeros((rows, META), jnp.float32)
    for k in range(top):
        named += jnp.where(lane == routes[:, k : k + 1], 1.0, 0.0)
    before = lax.broadcasted_iota(jnp.int32, (rows, rows), 0) > lax.broadcasted_iota(
        jnp.int32, (rows, rows), 1
    )
    earlier = jnp.dot(
        before.astype(jnp.float32).astype(jnp.bfloat16),
        named.astype(jnp.bfloat16),
        preferred_element_type=jnp.float32,
    )
    logits = logits_ref[...]
    powers = jnp.exp(logits - jnp.max(logits, axis=-1, keepdims=True))
    weights = powers / jnp.sum(powers, axis=-1, keepdims=True)
    high = weights.astype(jnp.bfloat16).astype(jnp.float32)
    low = weights - high
    meta = jnp.zeros((rows, META), jnp.float32)
    for k in range(top):
        hit = lane == routes[:, k : k + 1]
        rank = jnp.sum(jnp.where(hit, earlier, 0.0), axis=-1, keepdims=True)
        key = routes[:, k : k + 1].astype(jnp.float32) * cap + rank
        meta = jnp.where(lane == k, key, meta)
        meta = jnp.where(lane == top + k, high[:, k : k + 1], meta)
        meta = jnp.where(lane == 2 * top + k, low[:, k : k + 1], meta)
    out_ref[:, width:] = meta.astype(jnp.bfloat16)


def hand_on(chips, cap, top, place_ref, *refs):
    sources, refs = refs[:6], refs[6:]
    blocks, (high_ref, low_ref, all_ref) = refs[:6], refs[6:]
    rows = sources[0].shape[0]
    width = blocks[0].shape[1]
    z, c = place_ref[0], place_ref[1]
    near = 6 * cap
    slots = len(NEAR) * near + 2 * cap
    col = lax.broadcasted_iota(jnp.int32, (1, slots), 1)
    block = sum((col >= near * i).astype(jnp.int32) for i in range(1, len(NEAR) + 1))
    inside = col - block * near
    source = sum((inside >= cap * i).astype(jnp.int32) for i in range(1, 6))
    slot = inside - source * cap
    across = block == len(NEAR)
    source = jnp.where(across, source + jnp.where(c == 0, 2, 4), source)
    step = jnp.where(across, jnp.where(c == 0, 3, -3), block + NEAR[0])
    chip = z + step
    chip = jnp.where(chip < 0, chip + chips, chip)
    chip = jnp.where(chip >= chips, chip - chips, chip)
    target = ((2 * chip + c) * cap + slot + source * 2 * chips * cap).astype(jnp.float32)
    for s in range(6):
        all_ref[s * rows : (s + 1) * rows, :] = sources[s][...]
    meta = all_ref[:, width:].astype(jnp.float32)
    offset = (lax.broadcasted_iota(jnp.int32, (6 * rows, 1), 0) // rows * (2 * chips * cap)).astype(
        jnp.float32
    )
    pick = jnp.zeros((6 * rows, slots), jnp.float32)
    high, low = pick, pick
    for k in range(top):
        hit = meta[:, k : k + 1] + offset == target
        pick = jnp.where(hit, 1.0, pick)
        high = jnp.where(hit, meta[:, top + k : top + k + 1], high)
        low = jnp.where(hit, meta[:, 2 * top + k : 2 * top + k + 1], low)
    high_ref[...] = high.astype(jnp.bfloat16)
    low_ref[...] = low.astype(jnp.bfloat16)
    taken = lax.dot_general(
        pick.astype(jnp.bfloat16),
        all_ref[:, :width],
        (((0,), (0,)), ((), ())),
        preferred_element_type=jnp.float32,
    ).astype(jnp.bfloat16)
    for i in range(len(NEAR)):
        blocks[i][...] = taken[i * near : (i + 1) * near]
    blocks[5][...] = taken[len(NEAR) * near :]


def experts(tile, *refs):
    blocks, (gate_ref, up_ref, down_ref), refs = refs[:6], refs[6:9], refs[9:]
    outs, (x_ref, total_ref) = refs[:6], refs[6:]
    at = 0
    for b in blocks:
        x_ref[at : at + b.shape[0], :] = b[...]
        at += b.shape[0]
    hidden = gate_ref.shape[1]
    total_ref[...] = jnp.zeros_like(total_ref)

    @pl.loop(0, hidden // tile)
    def _(i):
        cols = pl.ds(pl.multiple_of(i * tile, tile), tile)
        x = x_ref[...]
        gate = jnp.minimum(jnp.dot(x, gate_ref[:, cols], preferred_element_type=jnp.float32), 7.0)
        upper = jnp.clip(
            jnp.dot(x, up_ref[:, cols], preferred_element_type=jnp.float32), -7.0, 7.0
        )
        active = (gate * jax.nn.sigmoid(1.702 * gate) * (upper + 1.0)).astype(jnp.bfloat16)
        total_ref[...] += jnp.dot(active, down_ref[cols, :], preferred_element_type=jnp.float32)

    at = 0
    for o in outs:
        o[...] = total_ref[at : at + o.shape[0], :].astype(jnp.bfloat16)
        at += o.shape[0]


def weigh(*refs):
    blocks, (high_ref, low_ref), refs = refs[:6], refs[6:8], refs[8:]
    far_mine, far_other, mine, other, x_ref = refs
    at = 0
    for b in blocks:
        x_ref[at : at + b.shape[0], :] = b[...]
        at += b.shape[0]
    x = x_ref[...]
    total = jnp.dot(high_ref[...], x, preferred_element_type=jnp.float32)
    total += jnp.dot(low_ref[...], x, preferred_element_type=jnp.float32)
    rows = mine.shape[0]
    mine[...] = total[:rows]
    other[...] = total[rows : 2 * rows].astype(jnp.bfloat16)
    for i in range(2):
        far_mine[i * rows : (i + 1) * rows, :] = total[(2 + 2 * i) * rows : (3 + 2 * i) * rows]
        far_other[i * rows : (i + 1) * rows, :] = total[
            (3 + 2 * i) * rows : (4 + 2 * i) * rows
        ].astype(jnp.bfloat16)


def join(mine, other, one, two):
    rows = one.shape[0]
    total = mine[...] + other[...].astype(jnp.float32)
    one[...] = total[:rows].astype(jnp.bfloat16)
    two[...] = total[rows:].astype(jnp.bfloat16)


def finish(mine, other, one, two, out):
    total = mine[...] + other[...].astype(jnp.float32)
    total += one[...].astype(jnp.float32) + two[...].astype(jnp.float32)
    out[...] = total.astype(jnp.bfloat16)


def shards(tokens, norm_gain, routes, route_logits, w_gate, w_up, w_down):
    rows, width = tokens.shape
    top = routes.shape[1]
    chips = lax.axis_size("z")
    cap = max(2, 2 * rows * top // (2 * chips))
    hidden = w_gate.shape[2]
    bf16 = lambda *shape: jax.ShapeDtypeStruct(shape, jnp.bfloat16)
    f32 = lambda *shape: jax.ShapeDtypeStruct(shape, jnp.float32)

    def shift(x, by):
        return lax.ppermute(x, "z", [(i, (i + by) % chips) for i in range(chips)])

    def across(x, sign):
        pairs = []
        for i in range(chips):
            pairs.append((2 * i, (i + 3 * sign) % chips * 2))
            pairs.append((2 * i + 1, (i - 3 * sign) % chips * 2 + 1))
        return lax.ppermute(x, ("z", "c"), pairs)

    def swap(x):
        return lax.ppermute(x, "c", [(0, 1), (1, 0)])

    place = jnp.stack([lax.axis_index("z"), lax.axis_index("c")]).astype(jnp.int32)
    own = call(functools.partial(prepare, cap), bf16(rows, width + META), 4)(
        tokens, norm_gain[None, :], routes, route_logits
    )
    low, high = shift(own, HOP), shift(own, -HOP)
    own2, low2, high2 = swap(own), swap(low), swap(high)
    near = 6 * cap
    slots = len(NEAR) * near + 2 * cap
    shapes = [bf16(near, width)] * len(NEAR) + [bf16(2 * cap, width)]
    weight = bf16(6 * rows, slots)
    *blocks, w_high, w_low = call(
        functools.partial(hand_on, chips, cap, top),
        shapes + [weight, weight],
        7,
        smem=1,
        scratch=[pltpu.VMEM((6 * rows, width + META), jnp.bfloat16)],
    )(place, own, own2, low, low2, high, high2)
    given = [shift(b, d) if d else b for b, d in zip(blocks, NEAR)] + [across(blocks[5], 1)]
    results = call(
        functools.partial(experts, 256),
        shapes,
        9,
        limit=56 << 20,
        scratch=[pltpu.VMEM((slots, width), jnp.bfloat16), pltpu.VMEM((slots, width), jnp.float32)],
        flops=6 * slots * width * hidden,
    )(*given, w_gate[0], w_up[0], w_down[0])
    back = [shift(b, -d) if d else b for b, d in zip(results, NEAR)] + [across(results[5], -1)]
    far_mine, far_other, mine, other = call(
        weigh,
        [f32(2 * rows, width), bf16(2 * rows, width), f32(rows, width), bf16(rows, width)],
        8,
        scratch=[pltpu.VMEM((slots, width), jnp.bfloat16)],
    )(*back, w_high, w_low)
    one, two = call(join, [bf16(rows, width)] * 2, 2)(far_mine, swap(far_other))
    return call(finish, bf16(rows, width), 4)(mine, swap(other), shift(one, -HOP), shift(two, HOP))


def solution(mesh):
    chips = mesh.shape["ep"] // 2
    split = Mesh(mesh.devices.reshape(mesh.shape["grp"], chips, 2), GRP_EP)
    ep = ("z", "c")
    placed = (
        P(GRP_EP, None),
        P(),
        P(GRP_EP, None),
        P(GRP_EP, None),
        P(ep, None, None),
        P(ep, None, None),
        P(ep, None, None),
    )
    return jax.shard_map(
        shards, mesh=split, in_specs=placed, out_specs=P(GRP_EP, None), check_vma=False
    )
```

```python
import functools

import jax
import jax.numpy as jnp
from jax import lax
from jax.experimental import pallas as pl
from jax.experimental.pallas import tpu as pltpu
from jax.sharding import Mesh
from jax.sharding import PartitionSpec as P

HOP = 5
NEAR = (-2, -1, 0, 1, 2)
GRP_EP = ("grp", "z", "c")
META = 128
LIMIT = 16 << 20
VMEM = pl.BlockSpec(memory_space=pltpu.VMEM)
SMEM = pl.BlockSpec(memory_space=pltpu.SMEM)


def call(body, out_shape, n_in, smem=0, limit=LIMIT, scratch=(), flops=1 << 20):
    return pl.pallas_call(
        body,
        out_shape=out_shape,
        in_specs=[SMEM] * smem + [VMEM] * (n_in - smem),
        scratch_shapes=scratch,
        compiler_params=pltpu.CompilerParams(vmem_limit_bytes=limit),
        cost_estimate=pl.CostEstimate(flops=flops, bytes_accessed=1 << 20, transcendentals=0),
    )


def prepare(cap, tok_hbm, gain_hbm, routes_hbm, logits_hbm, out_ref, *scratch):
    refs, sems = scratch[:4], scratch[4]
    copies = [
        pltpu.make_async_copy(source, ref, sems.at[i])
        for i, (source, ref) in enumerate(zip((tok_hbm, gain_hbm, routes_hbm, logits_hbm), refs))
    ]
    for copy in copies:
        copy.start()
    for copy in copies:
        copy.wait()
    tok_ref, gain_ref, routes_ref, logits_ref = refs
    rows, width = tok_ref.shape
    top = routes_ref.shape[0]
    x = tok_ref[...].astype(jnp.float32)
    scale = lax.rsqrt(jnp.mean(x * x, axis=-1, keepdims=True) + 1e-06)
    out_ref[:, :width] = (x * scale * gain_ref[...]).astype(jnp.bfloat16)
    lane = lax.broadcasted_iota(jnp.int32, (rows, META), 1).astype(jnp.float32)
    routes = jnp.transpose(routes_ref[...].astype(jnp.float32))
    logits = jnp.transpose(logits_ref[...])
    named = jnp.zeros((rows, META), jnp.float32)
    for k in range(top):
        named += jnp.where(lane == routes[:, k : k + 1], 1.0, 0.0)
    before = lax.broadcasted_iota(jnp.int32, (rows, rows), 0) > lax.broadcasted_iota(
        jnp.int32, (rows, rows), 1
    )
    earlier = jnp.dot(
        before.astype(jnp.float32).astype(jnp.bfloat16),
        named.astype(jnp.bfloat16),
        preferred_element_type=jnp.float32,
    )
    powers = jnp.exp(logits - jnp.max(logits, axis=-1, keepdims=True))
    weights = powers / jnp.sum(powers, axis=-1, keepdims=True)
    high = weights.astype(jnp.bfloat16).astype(jnp.float32)
    low = weights - high
    meta = jnp.zeros((rows, META), jnp.float32)
    for k in range(top):
        hit = lane == routes[:, k : k + 1]
        rank = jnp.sum(jnp.where(hit, earlier, 0.0), axis=-1, keepdims=True)
        key = routes[:, k : k + 1] * cap + rank
        meta = jnp.where(lane == k, key, meta)
        meta = jnp.where(lane == top + k, high[:, k : k + 1], meta)
        meta = jnp.where(lane == 2 * top + k, low[:, k : k + 1], meta)
    out_ref[:, width:] = meta.astype(jnp.bfloat16)


def hand_on(chips, cap, top, place_ref, *refs):
    sources, refs = refs[:6], refs[6:]
    blocks, (high_ref, low_ref, all_ref) = refs[:6], refs[6:]
    rows = sources[0].shape[0]
    width = blocks[0].shape[1]
    z, c = place_ref[0], place_ref[1]
    near = 6 * cap
    slots = len(NEAR) * near + 2 * cap
    col = lax.broadcasted_iota(jnp.int32, (1, slots), 1)
    block = sum((col >= near * i).astype(jnp.int32) for i in range(1, len(NEAR) + 1))
    inside = col - block * near
    source = sum((inside >= cap * i).astype(jnp.int32) for i in range(1, 6))
    slot = inside - source * cap
    across = block == len(NEAR)
    source = jnp.where(across, source + jnp.where(c == 0, 2, 4), source)
    step = jnp.where(across, jnp.where(c == 0, 3, -3), block + NEAR[0])
    chip = z + step
    chip = jnp.where(chip < 0, chip + chips, chip)
    chip = jnp.where(chip >= chips, chip - chips, chip)
    target = ((2 * chip + c) * cap + slot + source * 2 * chips * cap).astype(jnp.float32)
    for s in range(6):
        all_ref[s * rows : (s + 1) * rows, :] = sources[s][...]
    meta = all_ref[:, width:].astype(jnp.float32)
    offset = (lax.broadcasted_iota(jnp.int32, (6 * rows, 1), 0) // rows * (2 * chips * cap)).astype(
        jnp.float32
    )
    pick = jnp.zeros((6 * rows, slots), jnp.float32)
    high, low = pick, pick
    for k in range(top):
        hit = meta[:, k : k + 1] + offset == target
        pick = jnp.where(hit, 1.0, pick)
        high = jnp.where(hit, meta[:, top + k : top + k + 1], high)
        low = jnp.where(hit, meta[:, 2 * top + k : 2 * top + k + 1], low)
    high_ref[...] = high.astype(jnp.bfloat16)
    low_ref[...] = low.astype(jnp.bfloat16)
    taken = lax.dot_general(
        pick.astype(jnp.bfloat16),
        all_ref[:, :width],
        (((0,), (0,)), ((), ())),
        preferred_element_type=jnp.float32,
    ).astype(jnp.bfloat16)
    for i in range(len(NEAR)):
        blocks[i][...] = taken[i * near : (i + 1) * near]
    blocks[5][...] = taken[len(NEAR) * near :]


def experts(tile, *refs):
    blocks, (gate_ref, up_ref, down_ref), refs = refs[:6], refs[6:9], refs[9:]
    outs, (x_ref, total_ref) = refs[:6], refs[6:]
    at = 0
    for b in blocks:
        x_ref[at : at + b.shape[0], :] = b[...]
        at += b.shape[0]
    hidden = gate_ref.shape[1]
    total_ref[...] = jnp.zeros_like(total_ref)

    @pl.loop(0, hidden // tile)
    def _(i):
        cols = pl.ds(pl.multiple_of(i * tile, tile), tile)
        x = x_ref[...]
        gate = jnp.minimum(jnp.dot(x, gate_ref[:, cols], preferred_element_type=jnp.float32), 7.0)
        upper = jnp.clip(
            jnp.dot(x, up_ref[:, cols], preferred_element_type=jnp.float32), -7.0, 7.0
        )
        active = (gate * jax.nn.sigmoid(1.702 * gate) * (upper + 1.0)).astype(jnp.bfloat16)
        total_ref[...] += jnp.dot(active, down_ref[cols, :], preferred_element_type=jnp.float32)

    at = 0
    for o in outs:
        o[...] = total_ref[at : at + o.shape[0], :].astype(jnp.bfloat16)
        at += o.shape[0]


def weigh(*refs):
    blocks, (high_ref, low_ref), refs = refs[:6], refs[6:8], refs[8:]
    far_mine, far_other, mine, other, x_ref = refs
    at = 0
    for b in blocks:
        x_ref[at : at + b.shape[0], :] = b[...]
        at += b.shape[0]
    x = x_ref[...]
    total = jnp.dot(high_ref[...], x, preferred_element_type=jnp.float32)
    total += jnp.dot(low_ref[...], x, preferred_element_type=jnp.float32)
    rows = mine.shape[0]
    mine[...] = total[:rows]
    other[...] = total[rows : 2 * rows].astype(jnp.bfloat16)
    for i in range(2):
        far_mine[i * rows : (i + 1) * rows, :] = total[(2 + 2 * i) * rows : (3 + 2 * i) * rows]
        far_other[i * rows : (i + 1) * rows, :] = total[
            (3 + 2 * i) * rows : (4 + 2 * i) * rows
        ].astype(jnp.bfloat16)


def join(mine, other, one, two):
    rows = one.shape[0]
    total = mine[...] + other[...].astype(jnp.float32)
    one[...] = total[:rows].astype(jnp.bfloat16)
    two[...] = total[rows:].astype(jnp.bfloat16)


def finish(mine, other, one, two, out):
    total = mine[...] + other[...].astype(jnp.float32)
    total += one[...].astype(jnp.float32) + two[...].astype(jnp.float32)
    out[...] = total.astype(jnp.bfloat16)


def shards(tokens, norm_gain, routes, route_logits, w_gate, w_up, w_down):
    rows, width = tokens.shape
    top = routes.shape[1]
    chips = lax.axis_size("z")
    cap = max(2, 2 * rows * top // (2 * chips))
    hidden = w_gate.shape[2]
    bf16 = lambda *shape: jax.ShapeDtypeStruct(shape, jnp.bfloat16)
    f32 = lambda *shape: jax.ShapeDtypeStruct(shape, jnp.float32)

    def shift(x, by):
        return lax.ppermute(x, "z", [(i, (i + by) % chips) for i in range(chips)])

    def across(x, sign):
        pairs = []
        for i in range(chips):
            pairs.append((2 * i, (i + 3 * sign) % chips * 2))
            pairs.append((2 * i + 1, (i - 3 * sign) % chips * 2 + 1))
        return lax.ppermute(x, ("z", "c"), pairs)

    def swap(x):
        return lax.ppermute(x, "c", [(0, 1), (1, 0)])

    place = jnp.stack([lax.axis_index("z"), lax.axis_index("c")]).astype(jnp.int32)
    own = pl.pallas_call(
        functools.partial(prepare, cap),
        out_shape=pltpu.VMEM((rows, width + META), jnp.bfloat16),
        in_specs=[pl.BlockSpec(memory_space=pl.ANY)] * 4,
        out_specs=VMEM,
        scratch_shapes=[
            pltpu.VMEM((rows, width), jnp.bfloat16),
            pltpu.VMEM((1, width), jnp.float32),
            pltpu.VMEM((top, rows), jnp.int32),
            pltpu.VMEM((top, rows), jnp.float32),
            pltpu.SemaphoreType.DMA((4,)),
        ],
        compiler_params=pltpu.CompilerParams(vmem_limit_bytes=60 << 20),
        cost_estimate=pl.CostEstimate(flops=1 << 20, bytes_accessed=1 << 20, transcendentals=0),
    )(tokens, norm_gain[None, :], routes.T, route_logits.T)
    low, high = shift(own, HOP), shift(own, -HOP)
    own2, low2, high2 = swap(own), swap(low), swap(high)
    near = 6 * cap
    slots = len(NEAR) * near + 2 * cap
    shapes = [bf16(near, width)] * len(NEAR) + [bf16(2 * cap, width)]
    weight = bf16(6 * rows, slots)
    *blocks, w_high, w_low = call(
        functools.partial(hand_on, chips, cap, top),
        shapes + [weight, weight],
        7,
        smem=1,
        scratch=[pltpu.VMEM((6 * rows, width + META), jnp.bfloat16)],
        flops=4 * 6 * slots * width * hidden,
    )(place, own, own2, low, low2, high, high2)
    last = across(blocks[5], 1)
    given = [shift(b, d) if d else b for b, d in zip(blocks, NEAR)] + [last]
    results = call(
        functools.partial(experts, 256),
        shapes,
        9,
        limit=LIMIT,
        scratch=[pltpu.VMEM((slots, width), jnp.bfloat16), pltpu.VMEM((slots, width), jnp.float32)],
        flops=6 * slots * width * hidden,
    )(*given, w_gate[0], w_up[0], w_down[0])
    last = across(results[5], -1)
    back = [shift(b, -d) if d else b for b, d in zip(results, NEAR)] + [last]
    far_mine, far_other, mine, other = call(
        weigh,
        [f32(2 * rows, width), bf16(2 * rows, width), f32(rows, width), bf16(rows, width)],
        8,
        scratch=[pltpu.VMEM((slots, width), jnp.bfloat16)],
    )(*back, w_high, w_low)
    one, two = call(join, [bf16(rows, width)] * 2, 2)(far_mine, swap(far_other))
    return call(finish, bf16(rows, width), 4)(mine, swap(other), shift(one, -HOP), shift(two, HOP))


def solution(mesh):
    chips = mesh.shape["ep"] // 2
    split = Mesh(mesh.devices.reshape(mesh.shape["grp"], chips, 2), GRP_EP)
    ep = ("z", "c")
    placed = (
        P(GRP_EP, None),
        P(),
        P(GRP_EP, None),
        P(GRP_EP, None),
        P(ep, None, None),
        P(ep, None, None),
        P(ep, None, None),
    )
    return jax.shard_map(
        shards, mesh=split, in_specs=placed, out_specs=P(GRP_EP, None), check_vma=False
    )
```

```python
import functools

import jax
import jax.numpy as jnp
from jax import lax
from jax.experimental import pallas as pl
from jax.experimental.pallas import tpu as pltpu
from jax.sharding import Mesh
from jax.sharding import PartitionSpec as P

HOP = 5
NEAR = (-2, -1, 0, 1, 2)
GRP_EP = ("grp", "z", "c")
META = 128
LIMIT = 16 << 20
HEAVY = 12
VMEM = pl.BlockSpec(memory_space=pltpu.VMEM)
SMEM = pl.BlockSpec(memory_space=pltpu.SMEM)


def call(body, out_shape, n_in, smem=0, limit=LIMIT, scratch=(), flops=1 << 20):
    return pl.pallas_call(
        body,
        out_shape=out_shape,
        in_specs=[SMEM] * smem + [VMEM] * (n_in - smem),
        scratch_shapes=scratch,
        compiler_params=pltpu.CompilerParams(vmem_limit_bytes=limit),
        cost_estimate=pl.CostEstimate(flops=flops, bytes_accessed=1 << 20, transcendentals=0),
    )


def prepare(cap, tok_hbm, gain_hbm, routes_hbm, logits_hbm, out_ref, more_ref, *scratch):
    refs, sems = scratch[:4], scratch[4]
    copies = [
        pltpu.make_async_copy(source, ref, sems.at[i])
        for i, (source, ref) in enumerate(zip((tok_hbm, gain_hbm, routes_hbm, logits_hbm), refs))
    ]
    for copy in copies:
        copy.start()
    for copy in copies:
        copy.wait()
    tok_ref, gain_ref, routes_ref, logits_ref = refs
    rows, width = tok_ref.shape
    top = routes_ref.shape[0]
    x = tok_ref[...].astype(jnp.float32)
    scale = lax.rsqrt(jnp.mean(x * x, axis=-1, keepdims=True) + 1e-06)
    normed = (x * scale * gain_ref[...]).astype(jnp.bfloat16)
    half = more_ref.shape[1]
    out_ref[:, :half] = normed[:, :half]
    more_ref[...] = normed[:, half:]
    lane = lax.broadcasted_iota(jnp.int32, (rows, META), 1).astype(jnp.float32)
    routes = jnp.transpose(routes_ref[...].astype(jnp.float32))
    logits = jnp.transpose(logits_ref[...])
    named = jnp.zeros((rows, META), jnp.float32)
    for k in range(top):
        named += jnp.where(lane == routes[:, k : k + 1], 1.0, 0.0)
    before = lax.broadcasted_iota(jnp.int32, (rows, rows), 0) > lax.broadcasted_iota(
        jnp.int32, (rows, rows), 1
    )
    earlier = jnp.dot(
        before.astype(jnp.float32).astype(jnp.bfloat16),
        named.astype(jnp.bfloat16),
        preferred_element_type=jnp.float32,
    )
    powers = jnp.exp(logits - jnp.max(logits, axis=-1, keepdims=True))
    weights = powers / jnp.sum(powers, axis=-1, keepdims=True)
    high = weights.astype(jnp.bfloat16).astype(jnp.float32)
    low = weights - high
    meta = jnp.zeros((rows, META), jnp.float32)
    for k in range(top):
        hit = lane == routes[:, k : k + 1]
        rank = jnp.sum(jnp.where(hit, earlier, 0.0), axis=-1, keepdims=True)
        key = routes[:, k : k + 1] * cap + rank
        meta = jnp.where(lane == k, key, meta)
        meta = jnp.where(lane == top + k, high[:, k : k + 1], meta)
        meta = jnp.where(lane == 2 * top + k, low[:, k : k + 1], meta)
    out_ref[:, half:] = meta.astype(jnp.bfloat16)


def hand_on(chips, cap, top, place_ref, *refs):
    sources, refs = refs[:6], refs[6:]
    blocks, (high_ref, low_ref, pick_ref, all_ref) = refs[:6], refs[6:]
    rows = sources[0].shape[0]
    width = blocks[0].shape[1]
    z, c = place_ref[0], place_ref[1]
    near = 6 * cap
    slots = len(NEAR) * near + 2 * cap
    col = lax.broadcasted_iota(jnp.int32, (1, slots), 1)
    block = sum((col >= near * i).astype(jnp.int32) for i in range(1, len(NEAR) + 1))
    inside = col - block * near
    source = sum((inside >= cap * i).astype(jnp.int32) for i in range(1, 6))
    slot = inside - source * cap
    across = block == len(NEAR)
    source = jnp.where(across, source + jnp.where(c == 0, 2, 4), source)
    step = jnp.where(across, jnp.where(c == 0, 3, -3), block + NEAR[0])
    chip = z + step
    chip = jnp.where(chip < 0, chip + chips, chip)
    chip = jnp.where(chip >= chips, chip - chips, chip)
    target = ((2 * chip + c) * cap + slot + source * 2 * chips * cap).astype(jnp.float32)
    for s in range(6):
        all_ref[s * rows : (s + 1) * rows, :] = sources[s][...]
    meta = all_ref[:, width:].astype(jnp.float32)
    offset = (lax.broadcasted_iota(jnp.int32, (6 * rows, 1), 0) // rows * (2 * chips * cap)).astype(
        jnp.float32
    )
    pick = jnp.zeros((6 * rows, slots), jnp.float32)
    high, low = pick, pick
    for k in range(top):
        hit = meta[:, k : k + 1] + offset == target
        pick = jnp.where(hit, 1.0, pick)
        high = jnp.where(hit, meta[:, top + k : top + k + 1], high)
        low = jnp.where(hit, meta[:, 2 * top + k : 2 * top + k + 1], low)
    high_ref[...] = high.astype(jnp.bfloat16)
    low_ref[...] = low.astype(jnp.bfloat16)
    pick_ref[...] = pick.astype(jnp.bfloat16)
    take(pick_ref, all_ref, width, blocks)


def take(pick_ref, all_ref, width, blocks):
    taken = lax.dot_general(
        pick_ref[...],
        all_ref[:, :width],
        (((0,), (0,)), ((), ())),
        preferred_element_type=jnp.float32,
    ).astype(jnp.bfloat16)
    at = 0
    for b in blocks:
        b[...] = taken[at : at + b.shape[0]]
        at += b.shape[0]


def hand_more(pick_ref, *refs):
    sources, blocks, all_ref = refs[:6], refs[6:12], refs[12]
    rows, width = sources[0].shape
    for s in range(6):
        all_ref[s * rows : (s + 1) * rows, :] = sources[s][...]
    take(pick_ref, all_ref, width, blocks)


def gather(blocks, x_ref):
    at = 0
    for b in blocks:
        x_ref[at : at + b.shape[0], :] = b[...]
        at += b.shape[0]


def open_first(tile, *refs):
    blocks, (gate_ref, up_ref), (gate_out, up_out, x_ref) = refs[:6], refs[6:8], refs[8:]
    gather(blocks, x_ref)
    depth = x_ref.shape[1]

    @pl.loop(0, gate_ref.shape[1] // tile)
    def _(i):
        cols = pl.ds(pl.multiple_of(i * tile, tile), tile)
        x = x_ref[...]
        gate_out[:, cols] = jnp.dot(x, gate_ref[:depth, cols], preferred_element_type=jnp.float32)
        up_out[:, cols] = jnp.dot(x, up_ref[:depth, cols], preferred_element_type=jnp.float32)


def open_rest(tile, *refs):
    blocks, (gate_ref, up_ref, gate_in, up_in), (out_ref, x_ref) = refs[:6], refs[6:10], refs[10:]
    gather(blocks, x_ref)
    depth = x_ref.shape[1]

    @pl.loop(0, gate_ref.shape[1] // tile)
    def _(i):
        cols = pl.ds(pl.multiple_of(i * tile, tile), tile)
        x = x_ref[...]
        gate = gate_in[:, cols] + jnp.dot(
            x, gate_ref[depth:, cols], preferred_element_type=jnp.float32
        )
        upper = up_in[:, cols] + jnp.dot(
            x, up_ref[depth:, cols], preferred_element_type=jnp.float32
        )
        gate = jnp.minimum(gate, 7.0)
        upper = jnp.clip(upper, -7.0, 7.0)
        active = gate * jax.nn.sigmoid(1.702 * gate) * (upper + 1.0)
        out_ref[:, cols] = active.astype(jnp.bfloat16)


def close(start, tile, active_ref, down_ref, *outs):
    width = outs[0].shape[1]
    for j in range(0, width, tile):
        result = jnp.dot(
            active_ref[...],
            down_ref[:, start + j : start + j + tile],
            preferred_element_type=jnp.float32,
        ).astype(jnp.bfloat16)
        at = 0
        for o in outs:
            o[:, j : j + tile] = result[at : at + o.shape[0]]
            at += o.shape[0]


def weigh(*refs):
    blocks, (high_ref, low_ref), refs = refs[:6], refs[6:8], refs[8:]
    far_mine, far_other, mine, other, x_ref = refs
    gather(blocks, x_ref)
    x = x_ref[...]
    total = jnp.dot(high_ref[...], x, preferred_element_type=jnp.float32)
    total += jnp.dot(low_ref[...], x, preferred_element_type=jnp.float32)
    rows = mine.shape[0]
    mine[...] = total[:rows]
    other[...] = total[rows : 2 * rows].astype(jnp.bfloat16)
    for i in range(2):
        far_mine[i * rows : (i + 1) * rows, :] = total[(2 + 2 * i) * rows : (3 + 2 * i) * rows]
        far_other[i * rows : (i + 1) * rows, :] = total[
            (3 + 2 * i) * rows : (4 + 2 * i) * rows
        ].astype(jnp.bfloat16)


def join(mine, other, one, two):
    rows = one.shape[0]
    total = mine[...] + other[...].astype(jnp.float32)
    one[...] = total[:rows].astype(jnp.bfloat16)
    two[...] = total[rows:].astype(jnp.bfloat16)


def finish(*refs):
    out = refs[-1]
    at = 0
    for i in range(0, len(refs) - 1, 4):
        mine, other, one, two = refs[i : i + 4]
        total = mine[...] + other[...].astype(jnp.float32)
        total += one[...].astype(jnp.float32) + two[...].astype(jnp.float32)
        out[:, at : at + mine.shape[1]] = total.astype(jnp.bfloat16)
        at += mine.shape[1]


def shards(tokens, norm_gain, routes, route_logits, w_gate, w_up, w_down):
    rows, width = tokens.shape
    half = width // 2
    top = routes.shape[1]
    chips = lax.axis_size("z")
    cap = max(2, 2 * rows * top // (2 * chips))
    hidden = w_gate.shape[2]
    bf16 = lambda *shape: jax.ShapeDtypeStruct(shape, jnp.bfloat16)
    f32 = lambda *shape: jax.ShapeDtypeStruct(shape, jnp.float32)

    def shift(x, by):
        return lax.ppermute(x, "z", [(i, (i + by) % chips) for i in range(chips)])

    def across(x, sign):
        pairs = []
        for i in range(chips):
            pairs.append((2 * i, (i + 3 * sign) % chips * 2))
            pairs.append((2 * i + 1, (i - 3 * sign) % chips * 2 + 1))
        return lax.ppermute(x, ("z", "c"), pairs)

    def swap(x):
        return lax.ppermute(x, "c", [(0, 1), (1, 0)])

    def spread(blocks, sign):
        last = across(blocks[5], sign)
        return [shift(b, sign * d) if d else b for b, d in zip(blocks, NEAR)] + [last]

    place = jnp.stack([lax.axis_index("z"), lax.axis_index("c")]).astype(jnp.int32)
    own = pl.pallas_call(
        functools.partial(prepare, cap),
        out_shape=[
            pltpu.VMEM((rows, half + META), jnp.bfloat16),
            pltpu.VMEM((rows, half), jnp.bfloat16),
        ],
        in_specs=[pl.BlockSpec(memory_space=pl.ANY)] * 4,
        out_specs=[VMEM] * 2,
        scratch_shapes=[
            pltpu.VMEM((rows, width), jnp.bfloat16),
            pltpu.VMEM((1, width), jnp.float32),
            pltpu.VMEM((top, rows), jnp.int32),
            pltpu.VMEM((top, rows), jnp.float32),
            pltpu.SemaphoreType.DMA((4,)),
        ],
        compiler_params=pltpu.CompilerParams(vmem_limit_bytes=60 << 20),
        cost_estimate=pl.CostEstimate(flops=1 << 20, bytes_accessed=1 << 20, transcendentals=0),
    )(tokens, norm_gain[None, :], routes.T, route_logits.T)
    near = 6 * cap
    slots = len(NEAR) * near + 2 * cap
    work = 2 * slots * half * hidden
    shapes = [bf16(near, half)] * len(NEAR) + [bf16(2 * cap, half)]
    weight = bf16(6 * rows, slots)
    far = [(shift(x, HOP), shift(x, -HOP)) for x in own]
    mate = [swap(x) for x in own]
    parts = []
    for x, other, (low, high) in zip(own, mate, far):
        parts.append((x, other, low, swap(low), high, swap(high)))
    *first, w_high, w_low, pick = call(
        functools.partial(hand_on, chips, cap, top),
        shapes + [weight] * 3,
        7,
        smem=1,
        scratch=[pltpu.VMEM((6 * rows, half + META), jnp.bfloat16)],
        flops=HEAVY * work,
    )(place, *parts[0])
    first = spread(first, 1)
    second = call(
        hand_more, shapes, 7, scratch=[pltpu.VMEM((6 * rows, half), jnp.bfloat16)], flops=work // 8
    )(pick, *parts[1])
    second = spread(second, 1)
    x_half = pltpu.VMEM((slots, half), jnp.bfloat16)
    opened = call(
        functools.partial(open_first, 256), [f32(slots, hidden)] * 2, 8, scratch=[x_half], flops=2 * work
    )(*first, w_gate[0], w_up[0])
    active = call(
        functools.partial(open_rest, 256), bf16(slots, hidden), 10, scratch=[x_half], flops=2 * work
    )(*second, w_gate[0], w_up[0], *opened)
    mixed = []
    for start in (0, half):
        results = call(functools.partial(close, start, 256), shapes, 2, flops=work)(active, w_down[0])
        mixed.append(spread(results, -1))
    last = []
    for back in mixed:
        far_mine, far_other, mine, other = call(
            weigh,
            [f32(2 * rows, half), bf16(2 * rows, half), f32(rows, half), bf16(rows, half)],
            8,
            scratch=[x_half],
        )(*back, w_high, w_low)
        one, two = call(join, [bf16(rows, half)] * 2, 2)(far_mine, swap(far_other))
        last += [mine, swap(other), shift(one, -HOP), shift(two, HOP)]
    return call(finish, bf16(rows, width), 8)(*last)


def solution(mesh):
    chips = mesh.shape["ep"] // 2
    split = Mesh(mesh.devices.reshape(mesh.shape["grp"], chips, 2), GRP_EP)
    ep = ("z", "c")
    placed = (
        P(GRP_EP, None),
        P(),
        P(GRP_EP, None),
        P(GRP_EP, None),
        P(ep, None, None),
        P(ep, None, None),
        P(ep, None, None),
    )
    return jax.shard_map(
        shards, mesh=split, in_specs=placed, out_specs=P(GRP_EP, None), check_vma=False
    )
```

```python
import functools

import jax
import jax.numpy as jnp
from jax import lax
from jax.experimental import pallas as pl
from jax.experimental.pallas import tpu as pltpu
from jax.sharding import Mesh
from jax.sharding import PartitionSpec as P

HOP = 5
NEAR = (2, -2, 1, -1, 0)
GRP_EP = ("grp", "z", "c")
META = 128
LIMIT = 16 << 20
VMEM = pl.BlockSpec(memory_space=pltpu.VMEM)
SMEM = pl.BlockSpec(memory_space=pltpu.SMEM)


def call(body, out_shape, n_in, smem=0, limit=LIMIT, scratch=(), flops=1 << 20):
    return pl.pallas_call(
        body,
        out_shape=out_shape,
        in_specs=[SMEM] * smem + [VMEM] * (n_in - smem),
        scratch_shapes=scratch,
        compiler_params=pltpu.CompilerParams(vmem_limit_bytes=limit),
        cost_estimate=pl.CostEstimate(flops=flops, bytes_accessed=1 << 20, transcendentals=0),
    )


def prepare(cap, tok_hbm, gain_hbm, routes_hbm, logits_hbm, out_ref, *scratch):
    refs, sems = scratch[:4], scratch[4]
    copies = [
        pltpu.make_async_copy(source, ref, sems.at[i])
        for i, (source, ref) in enumerate(zip((tok_hbm, gain_hbm, routes_hbm, logits_hbm), refs))
    ]
    for copy in copies:
        copy.start()
    for copy in copies:
        copy.wait()
    tok_ref, gain_ref, routes_ref, logits_ref = refs
    rows, width = tok_ref.shape
    top = routes_ref.shape[0]
    x = tok_ref[...].astype(jnp.float32)
    scale = lax.rsqrt(jnp.mean(x * x, axis=-1, keepdims=True) + 1e-06)
    out_ref[:, :width] = (x * scale * gain_ref[...]).astype(jnp.bfloat16)
    lane = lax.broadcasted_iota(jnp.int32, (rows, META), 1).astype(jnp.float32)
    routes = jnp.transpose(routes_ref[...].astype(jnp.float32))
    logits = jnp.transpose(logits_ref[...])
    named = jnp.zeros((rows, META), jnp.float32)
    for k in range(top):
        named += jnp.where(lane == routes[:, k : k + 1], 1.0, 0.0)
    before = lax.broadcasted_iota(jnp.int32, (rows, rows), 0) > lax.broadcasted_iota(
        jnp.int32, (rows, rows), 1
    )
    earlier = jnp.dot(
        before.astype(jnp.float32).astype(jnp.bfloat16),
        named.astype(jnp.bfloat16),
        preferred_element_type=jnp.float32,
    )
    powers = jnp.exp(logits - jnp.max(logits, axis=-1, keepdims=True))
    weights = powers / jnp.sum(powers, axis=-1, keepdims=True)
    high = weights.astype(jnp.bfloat16).astype(jnp.float32)
    low = weights - high
    meta = jnp.zeros((rows, META), jnp.float32)
    for k in range(top):
        hit = lane == routes[:, k : k + 1]
        rank = jnp.sum(jnp.where(hit, earlier, 0.0), axis=-1, keepdims=True)
        key = routes[:, k : k + 1] * cap + rank
        meta = jnp.where(lane == k, key, meta)
        meta = jnp.where(lane == top + k, high[:, k : k + 1], meta)
        meta = jnp.where(lane == 2 * top + k, low[:, k : k + 1], meta)
    out_ref[:, width:] = meta.astype(jnp.bfloat16)


def hand_on(chips, cap, top, place_ref, *refs):
    sources, refs = refs[:6], refs[6:]
    blocks, (high_ref, low_ref, all_ref) = refs[:6], refs[6:]
    rows = sources[0].shape[0]
    width = blocks[0].shape[1]
    z, c = place_ref[0], place_ref[1]
    near = 6 * cap
    slots = len(NEAR) * near + 2 * cap
    col = lax.broadcasted_iota(jnp.int32, (1, slots), 1)
    block = sum((col >= near * i).astype(jnp.int32) for i in range(1, len(NEAR) + 1))
    inside = col - block * near
    source = sum((inside >= cap * i).astype(jnp.int32) for i in range(1, 6))
    slot = inside - source * cap
    across = block == len(NEAR)
    source = jnp.where(across, source + 2, source)
    step = sum(jnp.where(block == i, d, 0) for i, d in enumerate((*NEAR, 3)))
    chip = z + jnp.where(c == 0, step, -step)
    chip = jnp.where(chip < 0, chip + chips, chip)
    chip = jnp.where(chip >= chips, chip - chips, chip)
    target = ((2 * chip + c) * cap + slot + source * 2 * chips * cap).astype(jnp.float32)
    for s in range(6):
        all_ref[s * rows : (s + 1) * rows, :] = sources[s][...]
    meta = all_ref[:, width:].astype(jnp.float32)
    offset = (lax.broadcasted_iota(jnp.int32, (6 * rows, 1), 0) // rows * (2 * chips * cap)).astype(
        jnp.float32
    )
    pick = jnp.zeros((6 * rows, slots), jnp.float32)
    high, low = pick, pick
    for k in range(top):
        hit = meta[:, k : k + 1] + offset == target
        pick = jnp.where(hit, 1.0, pick)
        high = jnp.where(hit, meta[:, top + k : top + k + 1], high)
        low = jnp.where(hit, meta[:, 2 * top + k : 2 * top + k + 1], low)
    high_ref[...] = high.astype(jnp.bfloat16)
    low_ref[...] = low.astype(jnp.bfloat16)
    taken = lax.dot_general(
        pick.astype(jnp.bfloat16),
        all_ref[:, :width],
        (((0,), (0,)), ((), ())),
        preferred_element_type=jnp.float32,
    ).astype(jnp.bfloat16)
    for i in range(len(NEAR)):
        blocks[i][...] = taken[i * near : (i + 1) * near]
    blocks[5][...] = taken[len(NEAR) * near :]


def experts(tile, *refs):
    blocks, (gate_ref, up_ref, down_ref), refs = refs[:6], refs[6:9], refs[9:]
    outs, (x_ref, total_ref) = refs[:6], refs[6:]
    at = 0
    for b in blocks:
        x_ref[at : at + b.shape[0], :] = b[...]
        at += b.shape[0]
    hidden = gate_ref.shape[1]
    total_ref[...] = jnp.zeros_like(total_ref)

    @pl.loop(0, hidden // tile)
    def _(i):
        cols = pl.ds(pl.multiple_of(i * tile, tile), tile)
        x = x_ref[...]
        gate = jnp.minimum(jnp.dot(x, gate_ref[:, cols], preferred_element_type=jnp.float32), 7.0)
        upper = jnp.clip(
            jnp.dot(x, up_ref[:, cols], preferred_element_type=jnp.float32), -7.0, 7.0
        )
        active = (gate * jax.nn.sigmoid(1.702 * gate) * (upper + 1.0)).astype(jnp.bfloat16)
        total_ref[...] += jnp.dot(active, down_ref[cols, :], preferred_element_type=jnp.float32)

    at = 0
    for o in outs:
        o[...] = total_ref[at : at + o.shape[0], :].astype(jnp.bfloat16)
        at += o.shape[0]


def weigh(*refs):
    blocks, (high_ref, low_ref), refs = refs[:6], refs[6:8], refs[8:]
    far_mine, far_other, mine, other, x_ref = refs
    at = 0
    for b in blocks:
        x_ref[at : at + b.shape[0], :] = b[...]
        at += b.shape[0]
    x = x_ref[...]
    total = jnp.dot(high_ref[...], x, preferred_element_type=jnp.float32)
    total += jnp.dot(low_ref[...], x, preferred_element_type=jnp.float32)
    rows = mine.shape[0]
    mine[...] = total[:rows]
    other[...] = total[rows : 2 * rows].astype(jnp.bfloat16)
    for i in range(2):
        far_mine[i * rows : (i + 1) * rows, :] = total[(2 + 2 * i) * rows : (3 + 2 * i) * rows]
        far_other[i * rows : (i + 1) * rows, :] = total[
            (5 - 2 * i) * rows : (6 - 2 * i) * rows
        ].astype(jnp.bfloat16)


def join(mine, other, one, two):
    rows = one.shape[0]
    total = mine[...] + other[...].astype(jnp.float32)
    one[...] = total[:rows].astype(jnp.bfloat16)
    two[...] = total[rows:].astype(jnp.bfloat16)


def finish(mine, other, one, two, out):
    total = mine[...] + other[...].astype(jnp.float32)
    total += one[...].astype(jnp.float32) + two[...].astype(jnp.float32)
    out[...] = total.astype(jnp.bfloat16)


def shards(tokens, norm_gain, routes, route_logits, w_gate, w_up, w_down):
    rows, width = tokens.shape
    top = routes.shape[1]
    chips = lax.axis_size("z")
    cap = max(2, 2 * rows * top // (2 * chips))
    hidden = w_gate.shape[2]
    bf16 = lambda *shape: jax.ShapeDtypeStruct(shape, jnp.bfloat16)
    f32 = lambda *shape: jax.ShapeDtypeStruct(shape, jnp.float32)

    def shift(x, by):
        pairs = []
        for i in range(chips):
            pairs.append((2 * i, (i + by) % chips * 2))
            pairs.append((2 * i + 1, (i - by) % chips * 2 + 1))
        return lax.ppermute(x, ("z", "c"), pairs)

    def swap(x):
        return lax.ppermute(x, "c", [(0, 1), (1, 0)])

    place = jnp.stack([lax.axis_index("z"), lax.axis_index("c")]).astype(jnp.int32)
    own = pl.pallas_call(
        functools.partial(prepare, cap),
        out_shape=pltpu.VMEM((rows, width + META), jnp.bfloat16),
        in_specs=[pl.BlockSpec(memory_space=pl.ANY)] * 4,
        out_specs=VMEM,
        scratch_shapes=[
            pltpu.VMEM((rows, width), jnp.bfloat16),
            pltpu.VMEM((1, width), jnp.float32),
            pltpu.VMEM((top, rows), jnp.int32),
            pltpu.VMEM((top, rows), jnp.float32),
            pltpu.SemaphoreType.DMA((4,)),
        ],
        compiler_params=pltpu.CompilerParams(vmem_limit_bytes=60 << 20),
        cost_estimate=pl.CostEstimate(flops=1 << 20, bytes_accessed=1 << 20, transcendentals=0),
    )(tokens, norm_gain[None, :], routes.T, route_logits.T)
    low, high = shift(own, HOP), shift(own, -HOP)
    own2, high2, low2 = swap(own), swap(low), swap(high)
    near = 6 * cap
    slots = len(NEAR) * near + 2 * cap
    shapes = [bf16(near, width)] * len(NEAR) + [bf16(2 * cap, width)]
    weight = bf16(6 * rows, slots)
    *blocks, w_high, w_low = call(
        functools.partial(hand_on, chips, cap, top),
        shapes + [weight, weight],
        7,
        smem=1,
        scratch=[pltpu.VMEM((6 * rows, width + META), jnp.bfloat16)],
        flops=4 * 6 * slots * width * hidden,
    )(place, own, own2, low, low2, high, high2)
    last = shift(blocks[5], 3)
    given = [shift(b, d) if d else b for b, d in zip(blocks, NEAR)] + [last]
    results = call(
        functools.partial(experts, 256),
        shapes,
        9,
        limit=LIMIT,
        scratch=[pltpu.VMEM((slots, width), jnp.bfloat16), pltpu.VMEM((slots, width), jnp.float32)],
        flops=6 * slots * width * hidden,
    )(*given, w_gate[0], w_up[0], w_down[0])
    last = shift(results[5], -3)
    back = [shift(b, -d) if d else b for b, d in zip(results, NEAR)] + [last]
    far_mine, far_other, mine, other = call(
        weigh,
        [f32(2 * rows, width), bf16(2 * rows, width), f32(rows, width), bf16(rows, width)],
        8,
        scratch=[pltpu.VMEM((slots, width), jnp.bfloat16)],
    )(*back, w_high, w_low)
    one, two = call(join, [bf16(rows, width)] * 2, 2)(far_mine, swap(far_other))
    return call(finish, bf16(rows, width), 4)(mine, swap(other), shift(one, -HOP), shift(two, HOP))


def solution(mesh):
    chips = mesh.shape["ep"] // 2
    split = Mesh(mesh.devices.reshape(mesh.shape["grp"], chips, 2), GRP_EP)
    ep = ("z", "c")
    placed = (
        P(GRP_EP, None),
        P(),
        P(GRP_EP, None),
        P(GRP_EP, None),
        P(ep, None, None),
        P(ep, None, None),
        P(ep, None, None),
    )
    return jax.shard_map(
        shards, mesh=split, in_specs=placed, out_specs=P(GRP_EP, None), check_vma=False
    )
```

```python
import functools

import jax
import jax.numpy as jnp
from jax import lax
from jax.experimental import pallas as pl
from jax.experimental.pallas import tpu as pltpu
from jax.sharding import Mesh
from jax.sharding import PartitionSpec as P

HOP = 5
NEAR = (2, -2, 1, -1, 0)
GRP_EP = ("grp", "z", "c")
META = 128
LIMIT = 16 << 20
VMEM = pl.BlockSpec(memory_space=pltpu.VMEM)
SMEM = pl.BlockSpec(memory_space=pltpu.SMEM)


def call(body, out_shape, n_in, smem=0, limit=LIMIT, scratch=(), flops=1 << 20):
    return pl.pallas_call(
        body,
        out_shape=out_shape,
        in_specs=[SMEM] * smem + [VMEM] * (n_in - smem),
        scratch_shapes=scratch,
        compiler_params=pltpu.CompilerParams(vmem_limit_bytes=limit),
        cost_estimate=pl.CostEstimate(flops=flops, bytes_accessed=1 << 20, transcendentals=0),
    )


def prepare(cap, tok_hbm, gain_hbm, routes_hbm, logits_hbm, out_ref, *scratch):
    refs, sems = scratch[:4], scratch[4]
    copies = [
        pltpu.make_async_copy(source, ref, sems.at[i])
        for i, (source, ref) in enumerate(zip((tok_hbm, gain_hbm, routes_hbm, logits_hbm), refs))
    ]
    for copy in copies:
        copy.start()
    for copy in copies:
        copy.wait()
    tok_ref, gain_ref, routes_ref, logits_ref = refs
    rows, width = tok_ref.shape
    top = routes_ref.shape[0]
    x = tok_ref[...].astype(jnp.float32)
    scale = lax.rsqrt(jnp.mean(x * x, axis=-1, keepdims=True) + 1e-06)
    out_ref[:, :width] = (x * scale * gain_ref[...]).astype(jnp.bfloat16)
    lane = lax.broadcasted_iota(jnp.int32, (rows, META), 1).astype(jnp.float32)
    routes = jnp.transpose(routes_ref[...].astype(jnp.float32))
    logits = jnp.transpose(logits_ref[...])
    named = jnp.zeros((rows, META), jnp.float32)
    for k in range(top):
        named += jnp.where(lane == routes[:, k : k + 1], 1.0, 0.0)
    before = lax.broadcasted_iota(jnp.int32, (rows, rows), 0) > lax.broadcasted_iota(
        jnp.int32, (rows, rows), 1
    )
    earlier = jnp.dot(
        before.astype(jnp.float32).astype(jnp.bfloat16),
        named.astype(jnp.bfloat16),
        preferred_element_type=jnp.float32,
    )
    powers = jnp.exp(logits - jnp.max(logits, axis=-1, keepdims=True))
    weights = powers / jnp.sum(powers, axis=-1, keepdims=True)
    high = weights.astype(jnp.bfloat16).astype(jnp.float32)
    low = weights - high
    meta = jnp.zeros((rows, META), jnp.float32)
    for k in range(top):
        hit = lane == routes[:, k : k + 1]
        rank = jnp.sum(jnp.where(hit, earlier, 0.0), axis=-1, keepdims=True)
        key = routes[:, k : k + 1] * cap + rank
        meta = jnp.where(lane == k, key, meta)
        meta = jnp.where(lane == top + k, high[:, k : k + 1], meta)
        meta = jnp.where(lane == 2 * top + k, low[:, k : k + 1], meta)
    out_ref[:, width:] = meta.astype(jnp.bfloat16)


def hand_on(chips, cap, top, count, place_ref, *refs):
    sources, refs = refs[:count], refs[count:]
    blocks, (high_ref, low_ref, all_ref) = refs[:-3], refs[-3:]
    rows = sources[0].shape[0]
    width = blocks[0].shape[1]
    z, c = place_ref[0], place_ref[1]
    near = count * cap
    slots = high_ref.shape[1]
    col = lax.broadcasted_iota(jnp.int32, (1, slots), 1)
    block = sum((col >= near * i).astype(jnp.int32) for i in range(1, len(NEAR) + 1))
    inside = col - block * near
    source = sum((inside >= cap * i).astype(jnp.int32) for i in range(1, count))
    slot = inside - source * cap
    step = sum(jnp.where(block == i, d, 0) for i, d in enumerate((*NEAR, 3)))
    chip = z + jnp.where(c == 0, step, -step)
    chip = jnp.where(chip < 0, chip + chips, chip)
    chip = jnp.where(chip >= chips, chip - chips, chip)
    target = ((2 * chip + c) * cap + slot + source * 2 * chips * cap).astype(jnp.float32)
    for s in range(count):
        all_ref[s * rows : (s + 1) * rows, :] = sources[s][...]
    meta = all_ref[:, width:].astype(jnp.float32)
    index = lax.broadcasted_iota(jnp.int32, (count * rows, 1), 0) // rows
    offset = (index * (2 * chips * cap)).astype(jnp.float32)
    pick = jnp.zeros((count * rows, slots), jnp.float32)
    high, low = pick, pick
    for k in range(top):
        hit = meta[:, k : k + 1] + offset == target
        pick = jnp.where(hit, 1.0, pick)
        high = jnp.where(hit, meta[:, top + k : top + k + 1], high)
        low = jnp.where(hit, meta[:, 2 * top + k : 2 * top + k + 1], low)
    high_ref[...] = high.astype(jnp.bfloat16)
    low_ref[...] = low.astype(jnp.bfloat16)
    taken = lax.dot_general(
        pick.astype(jnp.bfloat16),
        all_ref[:, :width],
        (((0,), (0,)), ((), ())),
        preferred_element_type=jnp.float32,
    ).astype(jnp.bfloat16)
    at = 0
    for b in blocks:
        b[...] = taken[at : at + b.shape[0]]
        at += b.shape[0]


def gather(blocks, x_ref):
    at = 0
    for b in blocks:
        x_ref[at : at + b.shape[0], :] = b[...]
        at += b.shape[0]


def experts(tile, count, *refs):
    blocks, (gate_ref, up_ref, down_ref), refs = refs[:count], refs[count : count + 3], refs[count + 3 :]
    outs, (x_ref, total_ref) = refs[:count], refs[count:]
    gather(blocks, x_ref)
    hidden = gate_ref.shape[1]
    total_ref[...] = jnp.zeros_like(total_ref)

    @pl.loop(0, hidden // tile)
    def _(i):
        cols = pl.ds(pl.multiple_of(i * tile, tile), tile)
        x = x_ref[...]
        gate = jnp.minimum(jnp.dot(x, gate_ref[:, cols], preferred_element_type=jnp.float32), 7.0)
        upper = jnp.clip(
            jnp.dot(x, up_ref[:, cols], preferred_element_type=jnp.float32), -7.0, 7.0
        )
        active = (gate * jax.nn.sigmoid(1.702 * gate) * (upper + 1.0)).astype(jnp.bfloat16)
        total_ref[...] += jnp.dot(active, down_ref[cols, :], preferred_element_type=jnp.float32)

    at = 0
    for o in outs:
        o[...] = total_ref[at : at + o.shape[0], :].astype(jnp.bfloat16)
        at += o.shape[0]


def weighted(blocks, high_ref, low_ref, x_ref):
    gather(blocks, x_ref)
    x = x_ref[...]
    total = jnp.dot(high_ref[...], x, preferred_element_type=jnp.float32)
    return total + jnp.dot(low_ref[...], x, preferred_element_type=jnp.float32)


def weigh_near(*refs):
    mine, other, x_ref = refs[-3:]
    total = weighted(refs[:-5], *refs[-5:-3], x_ref)
    rows = mine.shape[0]
    mine[...] = total[:rows]
    other[...] = total[rows:].astype(jnp.bfloat16)


def weigh_far(*refs):
    mine, other, x_ref = refs[-3:]
    total = weighted(refs[:-5], *refs[-5:-3], x_ref)
    rows = mine.shape[0] // 2
    mine[:rows] = total[:rows]
    mine[rows:] = total[2 * rows : 3 * rows]
    other[:rows] = total[3 * rows :].astype(jnp.bfloat16)
    other[rows:] = total[rows : 2 * rows].astype(jnp.bfloat16)


def join(mine, other, one, two):
    rows = one.shape[0]
    total = mine[...] + other[...].astype(jnp.float32)
    one[...] = total[:rows].astype(jnp.bfloat16)
    two[...] = total[rows:].astype(jnp.bfloat16)


def finish(mine, other, one, two, out):
    total = mine[...] + other[...].astype(jnp.float32)
    total += one[...].astype(jnp.float32) + two[...].astype(jnp.float32)
    out[...] = total.astype(jnp.bfloat16)


def shards(tokens, norm_gain, routes, route_logits, w_gate, w_up, w_down):
    rows, width = tokens.shape
    top = routes.shape[1]
    chips = lax.axis_size("z")
    cap = max(2, 2 * rows * top // (2 * chips))
    hidden = w_gate.shape[2]
    bf16 = lambda *shape: jax.ShapeDtypeStruct(shape, jnp.bfloat16)
    f32 = lambda *shape: jax.ShapeDtypeStruct(shape, jnp.float32)

    def shift(x, by):
        pairs = []
        for i in range(chips):
            pairs.append((2 * i, (i + by) % chips * 2))
            pairs.append((2 * i + 1, (i - by) % chips * 2 + 1))
        return lax.ppermute(x, ("z", "c"), pairs)

    def swap(x):
        return lax.ppermute(x, "c", [(0, 1), (1, 0)])

    place = jnp.stack([lax.axis_index("z"), lax.axis_index("c")]).astype(jnp.int32)
    own = pl.pallas_call(
        functools.partial(prepare, cap),
        out_shape=pltpu.VMEM((rows, width + META), jnp.bfloat16),
        in_specs=[pl.BlockSpec(memory_space=pl.ANY)] * 4,
        out_specs=VMEM,
        scratch_shapes=[
            pltpu.VMEM((rows, width), jnp.bfloat16),
            pltpu.VMEM((1, width), jnp.float32),
            pltpu.VMEM((top, rows), jnp.int32),
            pltpu.VMEM((top, rows), jnp.float32),
            pltpu.SemaphoreType.DMA((4,)),
        ],
        compiler_params=pltpu.CompilerParams(vmem_limit_bytes=60 << 20),
        cost_estimate=pl.CostEstimate(flops=1 << 20, bytes_accessed=1 << 20, transcendentals=0),
    )(tokens, norm_gain[None, :], routes.T, route_logits.T)
    own2 = swap(own)
    low, high = shift(own, HOP), shift(own, -HOP)
    high2, low2 = swap(low), swap(high)
    steps = (*NEAR, 3)

    def hand(sources, sizes, flops):
        count = len(sources)
        weight = bf16(count * rows, sum(sizes))
        *blocks, w_high, w_low = call(
            functools.partial(hand_on, chips, cap, top, count),
            [bf16(n, width) for n in sizes] + [weight, weight],
            count + 1,
            smem=1,
            scratch=[pltpu.VMEM((count * rows, width + META), jnp.bfloat16)],
            flops=flops,
        )(place, *sources)
        return [shift(b, d) if d else b for b, d in zip(blocks, steps)], (w_high, w_low)

    def run(blocks):
        slots = sum(b.shape[0] for b in blocks)
        experts_of = call(
            functools.partial(experts, 256, len(blocks)),
            [bf16(*b.shape) for b in blocks],
            len(blocks) + 3,
            scratch=[pltpu.VMEM((slots, width), jnp.bfloat16), pltpu.VMEM((slots, width), jnp.float32)],
            flops=6 * slots * width * hidden,
        )
        return experts_of(*blocks, w_gate[0], w_up[0], w_down[0])

    def weigh(body, blocks, weights, rows):
        back = [shift(b, -d) if d else b for b, d in zip(blocks, steps)]
        slots = sum(b.shape[0] for b in blocks)
        sums_of = call(
            body,
            [f32(rows, width), bf16(rows, width)],
            len(back) + 2,
            scratch=[pltpu.VMEM((slots, width), jnp.bfloat16)],
        )
        return sums_of(*back, *weights)

    heavy = 24 * 256 * width * hidden
    near, near_weights = hand((own, own2), [2 * cap] * 5, heavy)
    far, far_weights = hand((low, low2, high, high2), [4 * cap] * 5 + [2 * cap], 1 << 28)
    near = run(near)
    far = run(far)
    mine, other = weigh(weigh_near, near, near_weights, rows)
    far_mine, far_other = weigh(weigh_far, far, far_weights, 2 * rows)
    one, two = call(join, [bf16(rows, width)] * 2, 2)(far_mine, swap(far_other))
    return call(finish, bf16(rows, width), 4)(mine, swap(other), shift(one, -HOP), shift(two, HOP))


def solution(mesh):
    chips = mesh.shape["ep"] // 2
    split = Mesh(mesh.devices.reshape(mesh.shape["grp"], chips, 2), GRP_EP)
    ep = ("z", "c")
    placed = (
        P(GRP_EP, None),
        P(),
        P(GRP_EP, None),
        P(GRP_EP, None),
        P(ep, None, None),
        P(ep, None, None),
        P(ep, None, None),
    )

    return jax.shard_map(
        shards, mesh=split, in_specs=placed, out_specs=P(GRP_EP, None), check_vma=False
    )
```

```python
import functools

import jax
import jax.numpy as jnp
from jax import lax
from jax.experimental import pallas as pl
from jax.experimental.pallas import tpu as pltpu
from jax.sharding import Mesh
from jax.sharding import PartitionSpec as P

HOP = 5
NEAR = (2, -2, 1, -1, 0)
EARLY = 2
GRP_EP = ("grp", "z", "c")
META = 128
LIMIT = 16 << 20
VMEM = pl.BlockSpec(memory_space=pltpu.VMEM)
SMEM = pl.BlockSpec(memory_space=pltpu.SMEM)


def call(body, out_shape, n_in, smem=0, limit=LIMIT, scratch=(), flops=1 << 20):
    return pl.pallas_call(
        body,
        out_shape=out_shape,
        in_specs=[SMEM] * smem + [VMEM] * (n_in - smem),
        scratch_shapes=scratch,
        compiler_params=pltpu.CompilerParams(vmem_limit_bytes=limit),
        cost_estimate=pl.CostEstimate(flops=flops, bytes_accessed=1 << 20, transcendentals=0),
    )


def prepare(cap, tok_hbm, gain_hbm, routes_hbm, logits_hbm, out_ref, *scratch):
    refs, sems = scratch[:4], scratch[4]
    copies = [
        pltpu.make_async_copy(source, ref, sems.at[i])
        for i, (source, ref) in enumerate(zip((tok_hbm, gain_hbm, routes_hbm, logits_hbm), refs))
    ]
    for copy in copies:
        copy.start()
    for copy in copies:
        copy.wait()
    tok_ref, gain_ref, routes_ref, logits_ref = refs
    rows, width = tok_ref.shape
    top = routes_ref.shape[0]
    x = tok_ref[...].astype(jnp.float32)
    scale = lax.rsqrt(jnp.mean(x * x, axis=-1, keepdims=True) + 1e-06)
    out_ref[:, :width] = (x * scale * gain_ref[...]).astype(jnp.bfloat16)
    lane = lax.broadcasted_iota(jnp.int32, (rows, META), 1).astype(jnp.float32)
    routes = jnp.transpose(routes_ref[...].astype(jnp.float32))
    logits = jnp.transpose(logits_ref[...])
    named = jnp.zeros((rows, META), jnp.float32)
    for k in range(top):
        named += jnp.where(lane == routes[:, k : k + 1], 1.0, 0.0)
    before = lax.broadcasted_iota(jnp.int32, (rows, rows), 0) > lax.broadcasted_iota(
        jnp.int32, (rows, rows), 1
    )
    earlier = jnp.dot(
        before.astype(jnp.float32).astype(jnp.bfloat16),
        named.astype(jnp.bfloat16),
        preferred_element_type=jnp.float32,
    )
    powers = jnp.exp(logits - jnp.max(logits, axis=-1, keepdims=True))
    weights = powers / jnp.sum(powers, axis=-1, keepdims=True)
    high = weights.astype(jnp.bfloat16).astype(jnp.float32)
    low = weights - high
    meta = jnp.zeros((rows, META), jnp.float32)
    for k in range(top):
        hit = lane == routes[:, k : k + 1]
        rank = jnp.sum(jnp.where(hit, earlier, 0.0), axis=-1, keepdims=True)
        key = routes[:, k : k + 1] * cap + rank
        meta = jnp.where(lane == k, key, meta)
        meta = jnp.where(lane == top + k, high[:, k : k + 1], meta)
        meta = jnp.where(lane == 2 * top + k, low[:, k : k + 1], meta)
    out_ref[:, width:] = meta.astype(jnp.bfloat16)


def hand_on(chips, cap, top, count, place_ref, *refs):
    sources, refs = refs[:count], refs[count:]
    blocks, (high_ref, low_ref, all_ref) = refs[:-3], refs[-3:]
    rows = sources[0].shape[0]
    width = blocks[0].shape[1]
    z, c = place_ref[0], place_ref[1]
    near = count * cap
    slots = high_ref.shape[1]
    col = lax.broadcasted_iota(jnp.int32, (1, slots), 1)
    block = sum((col >= near * i).astype(jnp.int32) for i in range(1, len(NEAR) + 1))
    inside = col - block * near
    source = sum((inside >= cap * i).astype(jnp.int32) for i in range(1, count))
    slot = inside - source * cap
    step = sum(jnp.where(block == i, d, 0) for i, d in enumerate((*NEAR, 3)))
    chip = z + jnp.where(c == 0, step, -step)
    chip = jnp.where(chip < 0, chip + chips, chip)
    chip = jnp.where(chip >= chips, chip - chips, chip)
    target = ((2 * chip + c) * cap + slot + source * 2 * chips * cap).astype(jnp.float32)
    for s in range(count):
        all_ref[s * rows : (s + 1) * rows, :] = sources[s][...]
    meta = all_ref[:, width:].astype(jnp.float32)
    index = lax.broadcasted_iota(jnp.int32, (count * rows, 1), 0) // rows
    offset = (index * (2 * chips * cap)).astype(jnp.float32)
    pick = jnp.zeros((count * rows, slots), jnp.float32)
    high, low = pick, pick
    for k in range(top):
        hit = meta[:, k : k + 1] + offset == target
        pick = jnp.where(hit, 1.0, pick)
        high = jnp.where(hit, meta[:, top + k : top + k + 1], high)
        low = jnp.where(hit, meta[:, 2 * top + k : 2 * top + k + 1], low)
    high_ref[...] = high.astype(jnp.bfloat16)
    low_ref[...] = low.astype(jnp.bfloat16)
    taken = lax.dot_general(
        pick.astype(jnp.bfloat16),
        all_ref[:, :width],
        (((0,), (0,)), ((), ())),
        preferred_element_type=jnp.float32,
    ).astype(jnp.bfloat16)
    at = 0
    for b in blocks:
        b[...] = taken[at : at + b.shape[0]]
        at += b.shape[0]


def gather(blocks, x_ref):
    at = 0
    for b in blocks:
        x_ref[at : at + b.shape[0], :] = b[...]
        at += b.shape[0]


def experts(tile, count, held, *refs):
    blocks, carried, refs = refs[:count], refs[count : count + held], refs[count + held :]
    (gate_ref, up_ref, down_ref), refs = refs[:3], refs[3:]
    outs, (x_ref, total_ref) = refs[:count], refs[count:]
    gather(blocks, x_ref)
    hidden = gate_ref.shape[1]
    total_ref[...] = jnp.zeros_like(total_ref)

    @pl.loop(0, hidden // tile)
    def _(i):
        cols = pl.ds(pl.multiple_of(i * tile, tile), tile)
        x = x_ref[...]
        gate = jnp.minimum(jnp.dot(x, gate_ref[:, cols], preferred_element_type=jnp.float32), 7.0)
        upper = jnp.clip(
            jnp.dot(x, up_ref[:, cols], preferred_element_type=jnp.float32), -7.0, 7.0
        )
        active = (gate * jax.nn.sigmoid(1.702 * gate) * (upper + 1.0)).astype(jnp.bfloat16)
        total_ref[...] += jnp.dot(active, down_ref[cols, :], preferred_element_type=jnp.float32)

    at = 0
    for i, (b, o) in enumerate(zip(blocks, outs)):
        o[: b.shape[0]] = total_ref[at : at + b.shape[0], :].astype(jnp.bfloat16)
        if EARLY <= i < EARLY + held:
            o[b.shape[0] :] = carried[i - EARLY][...]
        at += b.shape[0]


def weigh(*refs):
    early, blocks, refs = refs[:EARLY], refs[EARLY : EARLY + 6], refs[EARLY + 6 :]
    (high_ref, low_ref, near_high, near_low), refs = refs[:4], refs[4:]
    far_mine, far_other, mine, other, x_ref, near_ref = refs
    at, near_at, small = 0, 0, early[0].shape[0]
    for e in early:
        near_ref[near_at : near_at + small, :] = e[...]
        near_at += small
    for i, b in enumerate(blocks):
        both = EARLY <= i < len(NEAR)
        size = b.shape[0] - (small if both else 0)
        x_ref[at : at + size, :] = b[:size]
        at += size
        if both:
            near_ref[near_at : near_at + small, :] = b[size:]
            near_at += small
    x = x_ref[...]
    total = jnp.dot(high_ref[...], x, preferred_element_type=jnp.float32)
    total += jnp.dot(low_ref[...], x, preferred_element_type=jnp.float32)
    rows = mine.shape[0]
    far_mine[:rows] = total[:rows]
    far_mine[rows:] = total[2 * rows : 3 * rows]
    far_other[:rows] = total[3 * rows :].astype(jnp.bfloat16)
    far_other[rows:] = total[rows : 2 * rows].astype(jnp.bfloat16)
    x = near_ref[...]
    total = jnp.dot(near_high[...], x, preferred_element_type=jnp.float32)
    total += jnp.dot(near_low[...], x, preferred_element_type=jnp.float32)
    mine[...] = total[:rows]
    other[...] = total[rows:].astype(jnp.bfloat16)


def join(mine, other, one, two):
    rows = one.shape[0]
    total = mine[...] + other[...].astype(jnp.float32)
    one[...] = total[:rows].astype(jnp.bfloat16)
    two[...] = total[rows:].astype(jnp.bfloat16)


def finish(mine, other, one, two, out):
    total = mine[...] + other[...].astype(jnp.float32)
    total += one[...].astype(jnp.float32) + two[...].astype(jnp.float32)
    out[...] = total.astype(jnp.bfloat16)


def shards(tokens, norm_gain, routes, route_logits, w_gate, w_up, w_down):
    rows, width = tokens.shape
    top = routes.shape[1]
    chips = lax.axis_size("z")
    cap = max(2, 2 * rows * top // (2 * chips))
    hidden = w_gate.shape[2]
    bf16 = lambda *shape: jax.ShapeDtypeStruct(shape, jnp.bfloat16)
    f32 = lambda *shape: jax.ShapeDtypeStruct(shape, jnp.float32)

    def shift(x, by):
        pairs = []
        for i in range(chips):
            pairs.append((2 * i, (i + by) % chips * 2))
            pairs.append((2 * i + 1, (i - by) % chips * 2 + 1))
        return lax.ppermute(x, ("z", "c"), pairs)

    def swap(x):
        return lax.ppermute(x, "c", [(0, 1), (1, 0)])

    place = jnp.stack([lax.axis_index("z"), lax.axis_index("c")]).astype(jnp.int32)
    own = pl.pallas_call(
        functools.partial(prepare, cap),
        out_shape=pltpu.VMEM((rows, width + META), jnp.bfloat16),
        in_specs=[pl.BlockSpec(memory_space=pl.ANY)] * 4,
        out_specs=VMEM,
        scratch_shapes=[
            pltpu.VMEM((rows, width), jnp.bfloat16),
            pltpu.VMEM((1, width), jnp.float32),
            pltpu.VMEM((top, rows), jnp.int32),
            pltpu.VMEM((top, rows), jnp.float32),
            pltpu.SemaphoreType.DMA((4,)),
        ],
        compiler_params=pltpu.CompilerParams(vmem_limit_bytes=60 << 20),
        cost_estimate=pl.CostEstimate(flops=1 << 20, bytes_accessed=1 << 20, transcendentals=0),
    )(tokens, norm_gain[None, :], routes.T, route_logits.T)
    own2 = swap(own)
    low, high = shift(own, HOP), shift(own, -HOP)
    high2, low2 = swap(low), swap(high)
    steps = (*NEAR, 3)

    def hand(sources, sizes, flops):
        count = len(sources)
        weight = bf16(count * rows, sum(sizes))
        *blocks, w_high, w_low = call(
            functools.partial(hand_on, chips, cap, top, count),
            [bf16(n, width) for n in sizes] + [weight, weight],
            count + 1,
            smem=1,
            scratch=[pltpu.VMEM((count * rows, width + META), jnp.bfloat16)],
            flops=flops,
        )(place, *sources)
        return [shift(b, d) if d else b for b, d in zip(blocks, steps)], (w_high, w_low)

    def run(blocks, carried=()):
        slots = sum(b.shape[0] for b in blocks)
        sizes = [b.shape[0] for b in blocks]
        for i, b in enumerate(carried):
            sizes[EARLY + i] += b.shape[0]
        experts_of = call(
            functools.partial(experts, 256, len(blocks), len(carried)),
            [bf16(n, width) for n in sizes],
            len(blocks) + len(carried) + 3,
            scratch=[pltpu.VMEM((slots, width), jnp.bfloat16), pltpu.VMEM((slots, width), jnp.float32)],
            flops=6 * slots * width * hidden,
        )
        return experts_of(*blocks, *carried, w_gate[0], w_up[0], w_down[0])

    def back(blocks):
        return [shift(b, -d) if d else b for b, d in zip(blocks, steps)]

    heavy = 24 * 256 * width * hidden
    near, near_weights = hand((own, own2), [2 * cap] * 5, heavy)
    far, far_weights = hand((low, low2, high, high2), [4 * cap] * 5 + [2 * cap], 1 << 28)
    near = run(near)
    early = back(near[:EARLY])
    late = back(run(far, near[EARLY:]))
    far_mine, far_other, mine, other = call(
        weigh,
        [f32(2 * rows, width), bf16(2 * rows, width), f32(rows, width), bf16(rows, width)],
        EARLY + 10,
        scratch=[
            pltpu.VMEM((far_weights[0].shape[1], width), jnp.bfloat16),
            pltpu.VMEM((near_weights[0].shape[1], width), jnp.bfloat16),
        ],
    )(*early, *late, *far_weights, *near_weights)
    one, two = call(join, [bf16(rows, width)] * 2, 2)(far_mine, swap(far_other))
    return call(finish, bf16(rows, width), 4)(mine, swap(other), shift(one, -HOP), shift(two, HOP))


def solution(mesh):
    chips = mesh.shape["ep"] // 2
    split = Mesh(mesh.devices.reshape(mesh.shape["grp"], chips, 2), GRP_EP)
    ep = ("z", "c")
    placed = (
        P(GRP_EP, None),
        P(),
        P(GRP_EP, None),
        P(GRP_EP, None),
        P(ep, None, None),
        P(ep, None, None),
        P(ep, None, None),
    )

    return jax.shard_map(
        shards, mesh=split, in_specs=placed, out_specs=P(GRP_EP, None), check_vma=False
    )
```

```python
import functools

import jax
import jax.numpy as jnp
from jax import lax
from jax.experimental import pallas as pl
from jax.experimental.pallas import tpu as pltpu
from jax.sharding import Mesh
from jax.sharding import PartitionSpec as P

HOP = 5
NEAR = (2, -2, 1, -1, 0)
GRP_EP = ("grp", "z", "c")
META = 128
LIMIT = 16 << 20
VMEM = pl.BlockSpec(memory_space=pltpu.VMEM)
SMEM = pl.BlockSpec(memory_space=pltpu.SMEM)


def call(body, out_shape, n_in, smem=0, limit=LIMIT, scratch=(), flops=1 << 20):
    return pl.pallas_call(
        body,
        out_shape=out_shape,
        in_specs=[SMEM] * smem + [VMEM] * (n_in - smem),
        scratch_shapes=scratch,
        compiler_params=pltpu.CompilerParams(vmem_limit_bytes=limit),
        cost_estimate=pl.CostEstimate(flops=flops, bytes_accessed=1 << 20, transcendentals=0),
    )


def prepare(cap, tok_hbm, gain_hbm, routes_hbm, logits_hbm, out_ref, *scratch):
    refs, sems = scratch[:4], scratch[4]
    copies = [
        pltpu.make_async_copy(source, ref, sems.at[i])
        for i, (source, ref) in enumerate(zip((tok_hbm, gain_hbm, routes_hbm, logits_hbm), refs))
    ]
    for copy in copies:
        copy.start()
    for copy in copies:
        copy.wait()
    tok_ref, gain_ref, routes_ref, logits_ref = refs
    rows, width = tok_ref.shape
    top = routes_ref.shape[0]
    x = tok_ref[...].astype(jnp.float32)
    scale = lax.rsqrt(jnp.mean(x * x, axis=-1, keepdims=True) + 1e-06)
    out_ref[:, :width] = (x * scale * gain_ref[...]).astype(jnp.bfloat16)
    lane = lax.broadcasted_iota(jnp.int32, (rows, META), 1).astype(jnp.float32)
    routes = jnp.transpose(routes_ref[...].astype(jnp.float32))
    logits = jnp.transpose(logits_ref[...])
    named = jnp.zeros((rows, META), jnp.float32)
    for k in range(top):
        named += jnp.where(lane == routes[:, k : k + 1], 1.0, 0.0)
    before = lax.broadcasted_iota(jnp.int32, (rows, rows), 0) > lax.broadcasted_iota(
        jnp.int32, (rows, rows), 1
    )
    earlier = jnp.dot(
        before.astype(jnp.float32).astype(jnp.bfloat16),
        named.astype(jnp.bfloat16),
        preferred_element_type=jnp.float32,
    )
    powers = jnp.exp(logits - jnp.max(logits, axis=-1, keepdims=True))
    weights = powers / jnp.sum(powers, axis=-1, keepdims=True)
    high = weights.astype(jnp.bfloat16).astype(jnp.float32)
    low = weights - high
    meta = jnp.zeros((rows, META), jnp.float32)
    for k in range(top):
        hit = lane == routes[:, k : k + 1]
        rank = jnp.sum(jnp.where(hit, earlier, 0.0), axis=-1, keepdims=True)
        key = routes[:, k : k + 1] * cap + rank
        meta = jnp.where(lane == k, key, meta)
        meta = jnp.where(lane == top + k, high[:, k : k + 1], meta)
        meta = jnp.where(lane == 2 * top + k, low[:, k : k + 1], meta)
    out_ref[:, width:] = meta.astype(jnp.bfloat16)


def hand_on(chips, cap, top, count, cross, place_ref, *refs):
    sources, refs = refs[:count], refs[count:]
    blocks, (high_ref, low_ref, all_ref) = refs[:-3], refs[-3:]
    rows = sources[0].shape[0]
    width = blocks[0].shape[1]
    z, c = place_ref[0], place_ref[1]
    near = count * cap
    slots = high_ref.shape[1]
    col = lax.broadcasted_iota(jnp.int32, (1, slots), 1)
    block = sum((col >= near * i).astype(jnp.int32) for i in range(1, len(NEAR) + 1))
    inside = col - block * near
    source = sum((inside >= cap * i).astype(jnp.int32) for i in range(1, count))
    slot = inside - source * cap
    step = sum(jnp.where(block == i, d, 0) for i, d in enumerate((*NEAR, 3)))
    chip = z + jnp.where(c == 0, step, -step)
    chip = jnp.where(chip < 0, chip + chips, chip)
    chip = jnp.where(chip >= chips, chip - chips, chip)
    source = jnp.where(block == len(NEAR), cross, source)
    target = ((2 * chip + c) * cap + slot + source * 2 * chips * cap).astype(jnp.float32)
    for s in range(count):
        all_ref[s * rows : (s + 1) * rows, :] = sources[s][...]
    meta = all_ref[:, width:].astype(jnp.float32)
    index = lax.broadcasted_iota(jnp.int32, (count * rows, 1), 0) // rows
    offset = (index * (2 * chips * cap)).astype(jnp.float32)
    pick = jnp.zeros((count * rows, slots), jnp.float32)
    high, low = pick, pick
    for k in range(top):
        hit = meta[:, k : k + 1] + offset == target
        pick = jnp.where(hit, 1.0, pick)
        high = jnp.where(hit, meta[:, top + k : top + k + 1], high)
        low = jnp.where(hit, meta[:, 2 * top + k : 2 * top + k + 1], low)
    high_ref[...] = high.astype(jnp.bfloat16)
    low_ref[...] = low.astype(jnp.bfloat16)
    taken = lax.dot_general(
        pick.astype(jnp.bfloat16),
        all_ref[:, :width],
        (((0,), (0,)), ((), ())),
        preferred_element_type=jnp.float32,
    ).astype(jnp.bfloat16)
    at = 0
    for b in blocks:
        b[...] = taken[at : at + b.shape[0]]
        at += b.shape[0]


def gather(blocks, x_ref):
    at = 0
    for b in blocks:
        x_ref[at : at + b.shape[0], :] = b[...]
        at += b.shape[0]


def experts(tile, counts, *refs):
    count = sum(counts)
    blocks, (gate_ref, up_ref, down_ref), refs = refs[:count], refs[count : count + 3], refs[count + 3 :]
    outs, (x_ref, total_ref) = refs[:-2], refs[-2:]
    gather(blocks, x_ref)
    hidden = gate_ref.shape[1]
    total_ref[...] = jnp.zeros_like(total_ref)

    @pl.loop(0, hidden // tile)
    def _(i):
        cols = pl.ds(pl.multiple_of(i * tile, tile), tile)
        x = x_ref[...]
        gate = jnp.minimum(jnp.dot(x, gate_ref[:, cols], preferred_element_type=jnp.float32), 7.0)
        upper = jnp.clip(
            jnp.dot(x, up_ref[:, cols], preferred_element_type=jnp.float32), -7.0, 7.0
        )
        active = (gate * jax.nn.sigmoid(1.702 * gate) * (upper + 1.0)).astype(jnp.bfloat16)
        total_ref[...] += jnp.dot(active, down_ref[cols, :], preferred_element_type=jnp.float32)

    at, filled = 0, [0] * len(outs)
    i = 0
    for group in counts:
        for j in range(group):
            size = blocks[i].shape[0]
            outs[j][filled[j] : filled[j] + size] = total_ref[at : at + size, :].astype(jnp.bfloat16)
            filled[j] += size
            at += size
            i += 1


def weigh(counts, *refs):
    blocks, refs = refs[: max(counts)], refs[max(counts) :]
    weights, refs = refs[: 2 * len(counts)], refs[2 * len(counts) :]
    outs, scratch = refs[: 2 * len(counts)], refs[2 * len(counts) :]
    taken = [0] * len(blocks)
    for g, count in enumerate(counts):
        high_ref, low_ref = weights[2 * g : 2 * g + 2]
        mine, other = outs[2 * g : 2 * g + 2]
        x_ref, rows = scratch[g], mine.shape[0]
        cap, at = x_ref.shape[0] // (2 * len(NEAR)), 0
        for j in range(count):
            size = 2 * cap if j < len(NEAR) else cap
            x_ref[at : at + size, :] = blocks[j][taken[j] : taken[j] + size]
            taken[j] += size
            at += size
        x = x_ref[...]
        total = jnp.dot(high_ref[...], x, preferred_element_type=jnp.float32)
        total += jnp.dot(low_ref[...], x, preferred_element_type=jnp.float32)
        mine[...] = total[:rows]
        other[...] = total[rows:].astype(jnp.bfloat16)


def join(mine, other, out):
    out[...] = (mine[...] + other[...].astype(jnp.float32)).astype(jnp.bfloat16)


def finish(mine, other, one, two, out):
    total = mine[...] + other[...].astype(jnp.float32)
    total += one[...].astype(jnp.float32) + two[...].astype(jnp.float32)
    out[...] = total.astype(jnp.bfloat16)


def shards(tokens, norm_gain, routes, route_logits, w_gate, w_up, w_down):
    rows, width = tokens.shape
    top = routes.shape[1]
    chips = lax.axis_size("z")
    cap = max(2, 2 * rows * top // (2 * chips))
    hidden = w_gate.shape[2]
    bf16 = lambda *shape: jax.ShapeDtypeStruct(shape, jnp.bfloat16)
    f32 = lambda *shape: jax.ShapeDtypeStruct(shape, jnp.float32)

    def shift(x, by):
        pairs = []
        for i in range(chips):
            pairs.append((2 * i, (i + by) % chips * 2))
            pairs.append((2 * i + 1, (i - by) % chips * 2 + 1))
        return lax.ppermute(x, ("z", "c"), pairs)

    def swap(x):
        return lax.ppermute(x, "c", [(0, 1), (1, 0)])

    place = jnp.stack([lax.axis_index("z"), lax.axis_index("c")]).astype(jnp.int32)
    own = pl.pallas_call(
        functools.partial(prepare, cap),
        out_shape=pltpu.VMEM((rows, width + META), jnp.bfloat16),
        in_specs=[pl.BlockSpec(memory_space=pl.ANY)] * 4,
        out_specs=VMEM,
        scratch_shapes=[
            pltpu.VMEM((rows, width), jnp.bfloat16),
            pltpu.VMEM((1, width), jnp.float32),
            pltpu.VMEM((top, rows), jnp.int32),
            pltpu.VMEM((top, rows), jnp.float32),
            pltpu.SemaphoreType.DMA((4,)),
        ],
        compiler_params=pltpu.CompilerParams(vmem_limit_bytes=60 << 20),
        cost_estimate=pl.CostEstimate(flops=1 << 20, bytes_accessed=1 << 20, transcendentals=0),
    )(tokens, norm_gain[None, :], routes.T, route_logits.T)
    steps = (*NEAR, 3)

    def hand(sources, cross, flops):
        sizes = [2 * cap] * len(NEAR) + ([] if cross is None else [cap])
        weight = bf16(2 * rows, sum(sizes))
        hand_of = call(
            functools.partial(hand_on, chips, cap, top, 2, cross or 0),
            [bf16(n, width) for n in sizes] + [weight, weight],
            3,
            smem=1,
            scratch=[pltpu.VMEM((2 * rows, width + META), jnp.bfloat16)],
            flops=flops,
        )
        *blocks, w_high, w_low = hand_of(place, *sources)
        return [shift(b, d) if d else b for b, d in zip(blocks, steps)], (w_high, w_low)

    def run(*groups):
        counts = [len(g) for g in groups]
        blocks = [b for g in groups for b in g]
        slots = sum(b.shape[0] for b in blocks)
        sizes = [0] * max(counts)
        for g in groups:
            for j, b in enumerate(g):
                sizes[j] += b.shape[0]
        experts_of = call(
            functools.partial(experts, 256, counts),
            [bf16(n, width) for n in sizes],
            len(blocks) + 3,
            scratch=[pltpu.VMEM((slots, width), jnp.bfloat16), pltpu.VMEM((slots, width), jnp.float32)],
            flops=6 * slots * width * hidden,
        )
        results = experts_of(*blocks, w_gate[0], w_up[0], w_down[0])
        return [shift(b, -d) if d else b for b, d in zip(results, steps)]

    def sums(back, *weights):
        counts = [len(NEAR) + (w[0].shape[1] > 2 * cap * len(NEAR)) for w in weights]
        sums_of = call(
            functools.partial(weigh, counts),
            [f32(rows, width), bf16(rows, width)] * len(weights),
            len(back) + 2 * len(weights),
            scratch=[pltpu.VMEM((w[0].shape[1], width), jnp.bfloat16) for w in weights],
        )
        return sums_of(*back, *(w for pair in weights for w in pair))

    def home(mine, other, by):
        other = swap(other)
        total = call(join, bf16(rows, width), 2)(mine, other)
        return shift(total, by)

    own2 = swap(own)
    low = shift(own, HOP)
    high = shift(own, -HOP)
    high2 = swap(low)
    low2 = swap(high)
    near, near_weights = hand((own, own2), None, 24 * 256 * width * hidden)
    one, one_weights = hand((low, high2), 0, 1 << 26)
    two, two_weights = hand((high, low2), 1, 1 << 26)
    back_one = run(near, one)
    back_two = run(two)
    mine, other, one_mine, one_other = sums(back_one, near_weights, one_weights)
    two_mine, two_other = sums(back_two, two_weights)
    one = home(one_mine, one_other, -HOP)
    two = home(two_mine, two_other, HOP)
    other = swap(other)
    return call(finish, bf16(rows, width), 4)(mine, other, one, two)


def solution(mesh):
    chips = mesh.shape["ep"] // 2
    split = Mesh(mesh.devices.reshape(mesh.shape["grp"], chips, 2), GRP_EP)
    ep = ("z", "c")
    placed = (
        P(GRP_EP, None),
        P(),
        P(GRP_EP, None),
        P(GRP_EP, None),
        P(ep, None, None),
        P(ep, None, None),
        P(ep, None, None),
    )

    return jax.shard_map(
        shards, mesh=split, in_specs=placed, out_specs=P(GRP_EP, None), check_vma=False
    )
```

```python
import functools

import jax
import jax.numpy as jnp
from jax import lax
from jax.experimental import pallas as pl
from jax.experimental.pallas import tpu as pltpu
from jax.sharding import Mesh
from jax.sharding import PartitionSpec as P

HOP = 5
NEAR = (2, -2, 1, -1, 0)
EARLY = 2
GRP_EP = ("grp", "z", "c")
META = 128
LIMIT = 16 << 20
VMEM = pl.BlockSpec(memory_space=pltpu.VMEM)
SMEM = pl.BlockSpec(memory_space=pltpu.SMEM)


def call(body, out_shape, n_in, smem=0, limit=LIMIT, scratch=(), flops=1 << 20):
    return pl.pallas_call(
        body,
        out_shape=out_shape,
        in_specs=[SMEM] * smem + [VMEM] * (n_in - smem),
        scratch_shapes=scratch,
        compiler_params=pltpu.CompilerParams(vmem_limit_bytes=limit),
        cost_estimate=pl.CostEstimate(flops=flops, bytes_accessed=1 << 20, transcendentals=0),
    )


def prepare(cap, tok_hbm, gain_hbm, routes_hbm, logits_hbm, out_ref, *scratch):
    refs, sems = scratch[:4], scratch[4]
    copies = [
        pltpu.make_async_copy(source, ref, sems.at[i])
        for i, (source, ref) in enumerate(zip((tok_hbm, gain_hbm, routes_hbm, logits_hbm), refs))
    ]
    for copy in copies:
        copy.start()
    for copy in copies:
        copy.wait()
    tok_ref, gain_ref, routes_ref, logits_ref = refs
    rows, width = tok_ref.shape
    top = routes_ref.shape[0]
    x = tok_ref[...].astype(jnp.float32)
    scale = lax.rsqrt(jnp.mean(x * x, axis=-1, keepdims=True) + 1e-06)
    out_ref[:, :width] = (x * scale * gain_ref[...]).astype(jnp.bfloat16)
    lane = lax.broadcasted_iota(jnp.int32, (rows, META), 1).astype(jnp.float32)
    routes = jnp.transpose(routes_ref[...].astype(jnp.float32))
    logits = jnp.transpose(logits_ref[...])
    named = jnp.zeros((rows, META), jnp.float32)
    for k in range(top):
        named += jnp.where(lane == routes[:, k : k + 1], 1.0, 0.0)
    before = lax.broadcasted_iota(jnp.int32, (rows, rows), 0) > lax.broadcasted_iota(
        jnp.int32, (rows, rows), 1
    )
    earlier = jnp.dot(
        before.astype(jnp.float32).astype(jnp.bfloat16),
        named.astype(jnp.bfloat16),
        preferred_element_type=jnp.float32,
    )
    powers = jnp.exp(logits - jnp.max(logits, axis=-1, keepdims=True))
    weights = powers / jnp.sum(powers, axis=-1, keepdims=True)
    high = weights.astype(jnp.bfloat16).astype(jnp.float32)
    low = weights - high
    meta = jnp.zeros((rows, META), jnp.float32)
    for k in range(top):
        hit = lane == routes[:, k : k + 1]
        rank = jnp.sum(jnp.where(hit, earlier, 0.0), axis=-1, keepdims=True)
        key = routes[:, k : k + 1] * cap + rank
        meta = jnp.where(lane == k, key, meta)
        meta = jnp.where(lane == top + k, high[:, k : k + 1], meta)
        meta = jnp.where(lane == 2 * top + k, low[:, k : k + 1], meta)
    out_ref[:, width:] = meta.astype(jnp.bfloat16)


def hand_on(chips, cap, top, count, place_ref, *refs):
    sources, refs = refs[:count], refs[count:]
    blocks, (high_ref, low_ref, all_ref) = refs[:-3], refs[-3:]
    rows = sources[0].shape[0]
    width = blocks[0].shape[1]
    z, c = place_ref[0], place_ref[1]
    near = count * cap
    slots = high_ref.shape[1]
    col = lax.broadcasted_iota(jnp.int32, (1, slots), 1)
    block = sum((col >= near * i).astype(jnp.int32) for i in range(1, len(NEAR) + 1))
    inside = col - block * near
    source = sum((inside >= cap * i).astype(jnp.int32) for i in range(1, count))
    slot = inside - source * cap
    step = sum(jnp.where(block == i, d, 0) for i, d in enumerate((*NEAR, 3)))
    chip = z + jnp.where(c == 0, step, -step)
    chip = jnp.where(chip < 0, chip + chips, chip)
    chip = jnp.where(chip >= chips, chip - chips, chip)
    target = ((2 * chip + c) * cap + slot + source * 2 * chips * cap).astype(jnp.float32)
    for s in range(count):
        all_ref[s * rows : (s + 1) * rows, :] = sources[s][...]
    meta = all_ref[:, width:].astype(jnp.float32)
    index = lax.broadcasted_iota(jnp.int32, (count * rows, 1), 0) // rows
    offset = (index * (2 * chips * cap)).astype(jnp.float32)
    pick = jnp.zeros((count * rows, slots), jnp.float32)
    high, low = pick, pick
    for k in range(top):
        hit = meta[:, k : k + 1] + offset == target
        pick = jnp.where(hit, 1.0, pick)
        high = jnp.where(hit, meta[:, top + k : top + k + 1], high)
        low = jnp.where(hit, meta[:, 2 * top + k : 2 * top + k + 1], low)
    high_ref[...] = high.astype(jnp.bfloat16)
    low_ref[...] = low.astype(jnp.bfloat16)
    taken = lax.dot_general(
        pick.astype(jnp.bfloat16),
        all_ref[:, :width],
        (((0,), (0,)), ((), ())),
        preferred_element_type=jnp.float32,
    ).astype(jnp.bfloat16)
    at = 0
    for b in blocks:
        b[...] = taken[at : at + b.shape[0]]
        at += b.shape[0]


def gather(blocks, x_ref):
    at = 0
    for b in blocks:
        x_ref[at : at + b.shape[0], :] = b[...]
        at += b.shape[0]


def experts(tile, count, held, *refs):
    blocks, carried, refs = refs[:count], refs[count : count + held], refs[count + held :]
    (gate_ref, up_ref, down_ref), refs = refs[:3], refs[3:]
    outs, (x_ref, total_ref) = refs[:count], refs[count:]
    gather(blocks, x_ref)
    hidden = gate_ref.shape[1]
    total_ref[...] = jnp.zeros_like(total_ref)

    @pl.loop(0, hidden // tile)
    def _(i):
        cols = pl.ds(pl.multiple_of(i * tile, tile), tile)
        x = x_ref[...]
        gate = jnp.minimum(jnp.dot(x, gate_ref[:, cols], preferred_element_type=jnp.float32), 7.0)
        upper = jnp.clip(
            jnp.dot(x, up_ref[:, cols], preferred_element_type=jnp.float32), -7.0, 7.0
        )
        active = (gate * jax.nn.sigmoid(1.702 * gate) * (upper + 1.0)).astype(jnp.bfloat16)
        total_ref[...] += jnp.dot(active, down_ref[cols, :], preferred_element_type=jnp.float32)

    at = 0
    for i, (b, o) in enumerate(zip(blocks, outs)):
        o[: b.shape[0]] = total_ref[at : at + b.shape[0], :].astype(jnp.bfloat16)
        if EARLY <= i < EARLY + held:
            o[b.shape[0] :] = carried[i - EARLY][...]
        at += b.shape[0]


def weigh(*refs):
    early, blocks, refs = refs[:EARLY], refs[EARLY : EARLY + 6], refs[EARLY + 6 :]
    (high_ref, low_ref, near_high, near_low), refs = refs[:4], refs[4:]
    far_mine, far_other, mine, other, x_ref, near_ref = refs
    at, near_at, small = 0, 0, early[0].shape[0]
    for e in early:
        near_ref[near_at : near_at + small, :] = e[...]
        near_at += small
    for i, b in enumerate(blocks):
        both = EARLY <= i < len(NEAR)
        size = b.shape[0] - (small if both else 0)
        x_ref[at : at + size, :] = b[:size]
        at += size
        if both:
            near_ref[near_at : near_at + small, :] = b[size:]
            near_at += small
    x = x_ref[...]
    total = jnp.dot(high_ref[...], x, preferred_element_type=jnp.float32)
    total += jnp.dot(low_ref[...], x, preferred_element_type=jnp.float32)
    rows = mine.shape[0]
    far_mine[:rows] = total[:rows]
    far_mine[rows:] = total[2 * rows : 3 * rows]
    far_other[:rows] = total[3 * rows :].astype(jnp.bfloat16)
    far_other[rows:] = total[rows : 2 * rows].astype(jnp.bfloat16)
    x = near_ref[...]
    total = jnp.dot(near_high[...], x, preferred_element_type=jnp.float32)
    total += jnp.dot(near_low[...], x, preferred_element_type=jnp.float32)
    mine[...] = total[:rows]
    other[...] = total[rows:].astype(jnp.bfloat16)


def join(mine, other, one, two):
    rows = one.shape[0]
    total = mine[...] + other[...].astype(jnp.float32)
    one[...] = total[:rows].astype(jnp.bfloat16)
    two[...] = total[rows:].astype(jnp.bfloat16)


def finish(mine, other, one, two, out):
    total = mine[...] + other[...].astype(jnp.float32)
    total += one[...].astype(jnp.float32) + two[...].astype(jnp.float32)
    out[...] = total.astype(jnp.bfloat16)


def shards(tokens, norm_gain, routes, route_logits, w_gate, w_up, w_down):
    rows, width = tokens.shape
    top = routes.shape[1]
    chips = lax.axis_size("z")
    cap = max(2, 2 * rows * top // (2 * chips))
    hidden = w_gate.shape[2]
    bf16 = lambda *shape: jax.ShapeDtypeStruct(shape, jnp.bfloat16)
    f32 = lambda *shape: jax.ShapeDtypeStruct(shape, jnp.float32)

    def shift(x, by):
        pairs = []
        for i in range(chips):
            pairs.append((2 * i, (i + by) % chips * 2))
            pairs.append((2 * i + 1, (i - by) % chips * 2 + 1))
        return lax.ppermute(x, ("z", "c"), pairs)

    def swap(x):
        return lax.ppermute(x, "c", [(0, 1), (1, 0)])

    place = jnp.stack([lax.axis_index("z"), lax.axis_index("c")]).astype(jnp.int32)
    own = pl.pallas_call(
        functools.partial(prepare, cap),
        out_shape=pltpu.VMEM((rows, width + META), jnp.bfloat16),
        in_specs=[pl.BlockSpec(memory_space=pl.ANY)] * 4,
        out_specs=VMEM,
        scratch_shapes=[
            pltpu.VMEM((rows, width), jnp.bfloat16),
            pltpu.VMEM((1, width), jnp.float32),
            pltpu.VMEM((top, rows), jnp.int32),
            pltpu.VMEM((top, rows), jnp.float32),
            pltpu.SemaphoreType.DMA((4,)),
        ],
        compiler_params=pltpu.CompilerParams(vmem_limit_bytes=60 << 20),
        cost_estimate=pl.CostEstimate(flops=1 << 20, bytes_accessed=1 << 20, transcendentals=0),
    )(tokens, norm_gain[None, :], routes.T, route_logits.T)
    own2 = swap(own)
    low, high = shift(own, HOP), shift(own, -HOP)
    high2, low2 = swap(low), swap(high)
    steps = (*NEAR, 3)

    def spread(blocks, sign):
        moved = []
        for b, d in zip(blocks, steps):
            moved.append(shift(b, sign * d) if d else b)
        return moved

    def hand(sources, sizes, flops):
        count = len(sources)
        weight = bf16(count * rows, sum(sizes))
        *blocks, w_high, w_low = call(
            functools.partial(hand_on, chips, cap, top, count),
            [bf16(n, width) for n in sizes] + [weight, weight],
            count + 1,
            smem=1,
            scratch=[pltpu.VMEM((count * rows, width + META), jnp.bfloat16)],
            flops=flops,
        )(place, *sources)
        return spread(blocks, 1), (w_high, w_low)

    def run(blocks, carried=()):
        slots = sum(b.shape[0] for b in blocks)
        sizes = [b.shape[0] for b in blocks]
        for i, b in enumerate(carried):
            sizes[EARLY + i] += b.shape[0]
        experts_of = call(
            functools.partial(experts, hidden // 2, len(blocks), len(carried)),
            [bf16(n, width) for n in sizes],
            len(blocks) + len(carried) + 3,
            scratch=[pltpu.VMEM((slots, width), jnp.bfloat16), pltpu.VMEM((slots, width), jnp.float32)],
            flops=6 * slots * width * hidden,
        )
        return experts_of(*blocks, *carried, w_gate[0], w_up[0], w_down[0])

    def back(blocks):
        return spread(blocks, -1)

    heavy = 24 * 256 * width * hidden
    near, near_weights = hand((own, own2), [2 * cap] * 5, heavy)
    far, far_weights = hand((low, low2, high, high2), [4 * cap] * 5 + [2 * cap], 1 << 28)
    near = run(near)
    early = back(near[:EARLY])
    late = back(run(far, near[EARLY:]))
    far_mine, far_other, mine, other = call(
        weigh,
        [f32(2 * rows, width), bf16(2 * rows, width), f32(rows, width), bf16(rows, width)],
        EARLY + 10,
        scratch=[
            pltpu.VMEM((far_weights[0].shape[1], width), jnp.bfloat16),
            pltpu.VMEM((near_weights[0].shape[1], width), jnp.bfloat16),
        ],
    )(*early, *late, *far_weights, *near_weights)
    one, two = call(join, [bf16(rows, width)] * 2, 2)(far_mine, swap(far_other))
    return call(finish, bf16(rows, width), 4)(mine, swap(other), shift(one, -HOP), shift(two, HOP))


def solution(mesh):
    chips = mesh.shape["ep"] // 2
    split = Mesh(mesh.devices.reshape(mesh.shape["grp"], chips, 2), GRP_EP)
    ep = ("z", "c")
    placed = (
        P(GRP_EP, None),
        P(),
        P(GRP_EP, None),
        P(GRP_EP, None),
        P(ep, None, None),
        P(ep, None, None),
        P(ep, None, None),
    )

    return jax.shard_map(
        shards, mesh=split, in_specs=placed, out_specs=P(GRP_EP, None), check_vma=False
    )
```

```python
import functools

import jax
import jax.numpy as jnp
from jax import lax
from jax.experimental import pallas as pl
from jax.experimental.pallas import tpu as pltpu
from jax.sharding import Mesh
from jax.sharding import PartitionSpec as P

HOP = 5
NEAR = (2, -2, 1, -1, 0)
EARLY = 0
GRP_EP = ("grp", "z", "c")
META = 128
LIMIT = 16 << 20
VMEM = pl.BlockSpec(memory_space=pltpu.VMEM)
SMEM = pl.BlockSpec(memory_space=pltpu.SMEM)


def call(body, out_shape, n_in, smem=0, limit=LIMIT, scratch=(), flops=1 << 20):
    return pl.pallas_call(
        body,
        out_shape=out_shape,
        in_specs=[SMEM] * smem + [VMEM] * (n_in - smem),
        scratch_shapes=scratch,
        compiler_params=pltpu.CompilerParams(vmem_limit_bytes=limit),
        cost_estimate=pl.CostEstimate(flops=flops, bytes_accessed=1 << 20, transcendentals=0),
    )


def prepare(cap, tok_hbm, gain_hbm, routes_hbm, logits_hbm, out_ref, *scratch):
    refs, sems = scratch[:4], scratch[4]
    copies = [
        pltpu.make_async_copy(source, ref, sems.at[i])
        for i, (source, ref) in enumerate(zip((tok_hbm, gain_hbm, routes_hbm, logits_hbm), refs))
    ]
    for copy in copies:
        copy.start()
    for copy in copies:
        copy.wait()
    tok_ref, gain_ref, routes_ref, logits_ref = refs
    rows, width = tok_ref.shape
    top = routes_ref.shape[0]
    x = tok_ref[...].astype(jnp.float32)
    scale = lax.rsqrt(jnp.mean(x * x, axis=-1, keepdims=True) + 1e-06)
    out_ref[:, :width] = (x * scale * gain_ref[...]).astype(jnp.bfloat16)
    lane = lax.broadcasted_iota(jnp.int32, (rows, META), 1).astype(jnp.float32)
    routes = jnp.transpose(routes_ref[...].astype(jnp.float32))
    logits = jnp.transpose(logits_ref[...])
    named = jnp.zeros((rows, META), jnp.float32)
    for k in range(top):
        named += jnp.where(lane == routes[:, k : k + 1], 1.0, 0.0)
    before = lax.broadcasted_iota(jnp.int32, (rows, rows), 0) > lax.broadcasted_iota(
        jnp.int32, (rows, rows), 1
    )
    earlier = jnp.dot(
        before.astype(jnp.float32).astype(jnp.bfloat16),
        named.astype(jnp.bfloat16),
        preferred_element_type=jnp.float32,
    )
    powers = jnp.exp(logits - jnp.max(logits, axis=-1, keepdims=True))
    weights = powers / jnp.sum(powers, axis=-1, keepdims=True)
    high = weights.astype(jnp.bfloat16).astype(jnp.float32)
    low = weights - high
    meta = jnp.zeros((rows, META), jnp.float32)
    for k in range(top):
        hit = lane == routes[:, k : k + 1]
        rank = jnp.sum(jnp.where(hit, earlier, 0.0), axis=-1, keepdims=True)
        key = routes[:, k : k + 1] * cap + rank
        meta = jnp.where(lane == k, key, meta)
        meta = jnp.where(lane == top + k, high[:, k : k + 1], meta)
        meta = jnp.where(lane == 2 * top + k, low[:, k : k + 1], meta)
    out_ref[:, width:] = meta.astype(jnp.bfloat16)


def hand_on(chips, cap, top, count, place_ref, *refs):
    sources, refs = refs[:count], refs[count:]
    blocks, (high_ref, low_ref, all_ref) = refs[:-3], refs[-3:]
    rows = sources[0].shape[0]
    width = blocks[0].shape[1]
    z, c = place_ref[0], place_ref[1]
    near = count * cap
    slots = high_ref.shape[1]
    col = lax.broadcasted_iota(jnp.int32, (1, slots), 1)
    block = sum((col >= near * i).astype(jnp.int32) for i in range(1, len(NEAR) + 1))
    inside = col - block * near
    source = sum((inside >= cap * i).astype(jnp.int32) for i in range(1, count))
    slot = inside - source * cap
    step = sum(jnp.where(block == i, d, 0) for i, d in enumerate((*NEAR, 3)))
    chip = z + jnp.where(c == 0, step, -step)
    chip = jnp.where(chip < 0, chip + chips, chip)
    chip = jnp.where(chip >= chips, chip - chips, chip)
    target = ((2 * chip + c) * cap + slot + source * 2 * chips * cap).astype(jnp.float32)
    for s in range(count):
        all_ref[s * rows : (s + 1) * rows, :] = sources[s][...]
    meta = all_ref[:, width:].astype(jnp.float32)
    index = lax.broadcasted_iota(jnp.int32, (count * rows, 1), 0) // rows
    offset = (index * (2 * chips * cap)).astype(jnp.float32)
    pick = jnp.zeros((count * rows, slots), jnp.float32)
    high, low = pick, pick
    for k in range(top):
        hit = meta[:, k : k + 1] + offset == target
        pick = jnp.where(hit, 1.0, pick)
        high = jnp.where(hit, meta[:, top + k : top + k + 1], high)
        low = jnp.where(hit, meta[:, 2 * top + k : 2 * top + k + 1], low)
    high_ref[...] = high.astype(jnp.bfloat16)
    low_ref[...] = low.astype(jnp.bfloat16)
    taken = lax.dot_general(
        pick.astype(jnp.bfloat16),
        all_ref[:, :width],
        (((0,), (0,)), ((), ())),
        preferred_element_type=jnp.float32,
    ).astype(jnp.bfloat16)
    at = 0
    for b in blocks:
        b[...] = taken[at : at + b.shape[0]]
        at += b.shape[0]


def gather(blocks, x_ref):
    at = 0
    for b in blocks:
        x_ref[at : at + b.shape[0], :] = b[...]
        at += b.shape[0]


def experts(count, held, *refs):
    blocks, carried, refs = refs[:count], refs[count : count + held], refs[count + held :]
    (gate_ref, up_ref, down_ref), refs = refs[:3], refs[3:]
    outs, x_ref = refs[:count], refs[count]
    gather(blocks, x_ref)
    x = x_ref[...]
    gate = jnp.minimum(jnp.dot(x, gate_ref[...], preferred_element_type=jnp.float32), 7.0)
    upper = jnp.clip(jnp.dot(x, up_ref[...], preferred_element_type=jnp.float32), -7.0, 7.0)
    active = (gate * jax.nn.sigmoid(1.702 * gate) * (upper + 1.0)).astype(jnp.bfloat16)
    total = jnp.dot(active, down_ref[...], preferred_element_type=jnp.float32).astype(jnp.bfloat16)
    at = 0
    for i, (b, o) in enumerate(zip(blocks, outs)):
        o[: b.shape[0]] = total[at : at + b.shape[0]]
        if EARLY <= i < EARLY + held:
            o[b.shape[0] :] = carried[i - EARLY][...]
        at += b.shape[0]


def weigh(*refs):
    early, blocks, refs = refs[:EARLY], refs[EARLY : EARLY + 6], refs[EARLY + 6 :]
    (high_ref, low_ref, near_high, near_low), refs = refs[:4], refs[4:]
    far_mine, far_other, mine, other, x_ref, near_ref = refs
    at, near_at, small = 0, 0, near_ref.shape[0] // len(NEAR)
    for e in early:
        near_ref[near_at : near_at + small, :] = e[...]
        near_at += small
    for i, b in enumerate(blocks):
        both = EARLY <= i < len(NEAR)
        size = b.shape[0] - (small if both else 0)
        x_ref[at : at + size, :] = b[:size]
        at += size
        if both:
            near_ref[near_at : near_at + small, :] = b[size:]
            near_at += small
    x = x_ref[...]
    total = jnp.dot(high_ref[...], x, preferred_element_type=jnp.float32)
    total += jnp.dot(low_ref[...], x, preferred_element_type=jnp.float32)
    rows = mine.shape[0]
    far_mine[:rows] = total[:rows]
    far_mine[rows:] = total[2 * rows : 3 * rows]
    far_other[:rows] = total[3 * rows :].astype(jnp.bfloat16)
    far_other[rows:] = total[rows : 2 * rows].astype(jnp.bfloat16)
    x = near_ref[...]
    total = jnp.dot(near_high[...], x, preferred_element_type=jnp.float32)
    total += jnp.dot(near_low[...], x, preferred_element_type=jnp.float32)
    mine[...] = total[:rows]
    other[...] = total[rows:].astype(jnp.bfloat16)


def join(mine, other, one, two):
    rows = one.shape[0]
    total = mine[...] + other[...].astype(jnp.float32)
    one[...] = total[:rows].astype(jnp.bfloat16)
    two[...] = total[rows:].astype(jnp.bfloat16)


def finish(mine, other, one, two, out):
    total = mine[...] + other[...].astype(jnp.float32)
    total += one[...].astype(jnp.float32) + two[...].astype(jnp.float32)
    out[...] = total.astype(jnp.bfloat16)


def shards(tokens, norm_gain, routes, route_logits, w_gate, w_up, w_down):
    rows, width = tokens.shape
    top = routes.shape[1]
    chips = lax.axis_size("z")
    cap = max(2, 2 * rows * top // (2 * chips))
    hidden = w_gate.shape[2]
    bf16 = lambda *shape: jax.ShapeDtypeStruct(shape, jnp.bfloat16)
    f32 = lambda *shape: jax.ShapeDtypeStruct(shape, jnp.float32)

    def shift(x, by):
        pairs = []
        for i in range(chips):
            pairs.append((2 * i, (i + by) % chips * 2))
            pairs.append((2 * i + 1, (i - by) % chips * 2 + 1))
        return lax.ppermute(x, ("z", "c"), pairs)

    def swap(x):
        return lax.ppermute(x, "c", [(0, 1), (1, 0)])

    place = jnp.stack([lax.axis_index("z"), lax.axis_index("c")]).astype(jnp.int32)
    own = pl.pallas_call(
        functools.partial(prepare, cap),
        out_shape=pltpu.VMEM((rows, width + META), jnp.bfloat16),
        in_specs=[pl.BlockSpec(memory_space=pl.ANY)] * 4,
        out_specs=VMEM,
        scratch_shapes=[
            pltpu.VMEM((rows, width), jnp.bfloat16),
            pltpu.VMEM((1, width), jnp.float32),
            pltpu.VMEM((top, rows), jnp.int32),
            pltpu.VMEM((top, rows), jnp.float32),
            pltpu.SemaphoreType.DMA((4,)),
        ],
        compiler_params=pltpu.CompilerParams(vmem_limit_bytes=60 << 20),
        cost_estimate=pl.CostEstimate(flops=1 << 20, bytes_accessed=1 << 20, transcendentals=0),
    )(tokens, norm_gain[None, :], routes.T, route_logits.T)
    own2 = swap(own)
    low, high = shift(own, HOP), shift(own, -HOP)
    high2, low2 = swap(low), swap(high)
    steps = (*NEAR, 3)

    def spread(blocks, sign):
        moved = []
        for b, d in zip(blocks, steps):
            moved.append(shift(b, sign * d) if d else b)
        return moved

    def hand(sources, sizes, flops):
        count = len(sources)
        weight = bf16(count * rows, sum(sizes))
        *blocks, w_high, w_low = call(
            functools.partial(hand_on, chips, cap, top, count),
            [bf16(n, width) for n in sizes] + [weight, weight],
            count + 1,
            smem=1,
            scratch=[pltpu.VMEM((count * rows, width + META), jnp.bfloat16)],
            flops=flops,
        )(place, *sources)
        return spread(blocks, 1), (w_high, w_low)

    def run(blocks, carried=()):
        slots = sum(b.shape[0] for b in blocks)
        sizes = [b.shape[0] for b in blocks]
        for i, b in enumerate(carried):
            sizes[EARLY + i] += b.shape[0]
        experts_of = call(
            functools.partial(experts, len(blocks), len(carried)),
            [bf16(n, width) for n in sizes],
            len(blocks) + len(carried) + 3,
            scratch=[pltpu.VMEM((slots, width), jnp.bfloat16)],
            flops=6 * slots * width * hidden,
        )
        return experts_of(*blocks, *carried, w_gate[0], w_up[0], w_down[0])

    def back(blocks):
        return spread(blocks, -1)

    heavy = 24 * 256 * width * hidden
    near, near_weights = hand((own, own2), [2 * cap] * 5, heavy)
    far, far_weights = hand((low, low2, high, high2), [4 * cap] * 5 + [2 * cap], 1 << 28)
    near = run(near)
    early = back(near[:EARLY])
    late = back(run(far, near[EARLY:]))
    far_mine, far_other, mine, other = call(
        weigh,
        [f32(2 * rows, width), bf16(2 * rows, width), f32(rows, width), bf16(rows, width)],
        EARLY + 10,
        scratch=[
            pltpu.VMEM((far_weights[0].shape[1], width), jnp.bfloat16),
            pltpu.VMEM((near_weights[0].shape[1], width), jnp.bfloat16),
        ],
    )(*early, *late, *far_weights, *near_weights)
    one, two = call(join, [bf16(rows, width)] * 2, 2)(far_mine, swap(far_other))
    return call(finish, bf16(rows, width), 4)(mine, swap(other), shift(one, -HOP), shift(two, HOP))


def solution(mesh):
    chips = mesh.shape["ep"] // 2
    split = Mesh(mesh.devices.reshape(mesh.shape["grp"], chips, 2), GRP_EP)
    ep = ("z", "c")
    placed = (
        P(GRP_EP, None),
        P(),
        P(GRP_EP, None),
        P(GRP_EP, None),
        P(ep, None, None),
        P(ep, None, None),
        P(ep, None, None),
    )

    return jax.shard_map(
        shards, mesh=split, in_specs=placed, out_specs=P(GRP_EP, None), check_vma=False
    )
```
